512 devices in a mesh: rep: 2 (over z_hi), fs: 32 (over z_lo, y), tp: 8 (over x, core).
Axes of the slice: x: 4, y: 4, z: 16 (z_hi: 2, z_lo: 8; z = z_hi * 8 + z_lo), core: 2. Of those that a mesh axis runs over, the one named last changes fastest.
Arguments:
- inputs: bfloat16 [32768, 2048], P(('rep', 'fs')), may hold values from -6 to 6
- gain: float32 [2048], replicated, may hold values from 0.1 to 1.9
- gate_weight: bfloat16 [2048, 3072], P('fs', 'tp'), may hold values from -0.125 to 0.125
- up_weight: bfloat16 [2048, 3072], P('fs', 'tp'), may hold values from -0.125 to 0.125
- down_weight: bfloat16 [2048, 3072], P('fs', 'tp'), may hold values from -0.109375 to 0.109375
- cotangent: bfloat16 [32768, 2048], P(('rep', 'fs')), may hold values from -16 to 16
Outputs:
- input_gradient: bfloat16 [32768, 2048], P(('rep', 'fs'))
- gain_gradient: float32 [2048], replicated
- d_down: float32 [2048, 3072], P('fs', 'tp')
The draws below stay inside these ranges and needn't reach their ends.
All inputs are finite; a program needn't handle non-finite values.
Results may differ from the reference program's by a relative error of at most 0.014.
Values may be sent and summed in bfloat16 or wider, within the bound.
No kernel may reach another device: no remote copies, remote signals or barrier semaphores. Data moves between devices by JAX's collectives and lax.ppermute only.
A program may use at most 64 MiB of HBM per device.

```python
import jax
import jax.numpy as jnp
from jax import lax

D = 2048
FF = 3072
TOKENS = 32768
N_TP = 8


def with_spikes(result, stream_key, source, target, blocks, factor):
    owner, partner = [(jnp.arange(result.shape[dim]) // (result.shape[dim] // blocks)).reshape([-1 if axis == dim else 1 for axis in range(result.ndim)]) for dim in (source, target)]
    chosen = jax.random.permutation(stream_key, blocks)[partner]
    strong = (owner == chosen) | (owner == (partner + blocks // 2) % blocks)
    return jnp.where(strong, factor * result, result)


def shard_levels(rng, dims, split, least, high):
    def one(dim, parts):
        steps = jax.random.uniform(jax.random.fold_in(jax.random.fold_in(rng, 6), dim), (parts,), jnp.float32, least / len(split), high / len(split))
        return jnp.repeat(jnp.exp(steps), dims[dim] // parts).reshape((-1,) + (1,) * (len(dims) - dim - 1))

    factor_of = one(*split[0])
    for cut in split[1:]:
        factor_of = factor_of * one(*cut)
    return factor_of


def gaussian(rng, shape, width, bound, split=(), dtype=jnp.bfloat16):
    drawn = width * jax.random.normal(rng, shape, jnp.float32)
    if split:
        drawn = drawn * shard_levels(rng, shape, split, -0.22, 0.18)
    return jnp.clip(drawn, -bound, bound).astype(dtype)


def bell_draw_with(stream_key, extent, scale, reach, cuts, heavy, held_as=jnp.bfloat16):
    array = scale * jax.random.normal(stream_key, extent, jnp.float32)
    if cuts:
        array = array * shard_levels(stream_key, extent, cuts, -0.22, 0.18)
    return jnp.clip(with_spikes(array, jax.random.fold_in(stream_key, 3), *heavy), -reach, reach).astype(held_as)


def setup_inputs(seed: int = 0) -> dict:
    key_of = jax.random.split(jax.random.key(seed), 7)
    inputs = gaussian(key_of[0], (TOKENS, D), 1.0, 6.0, ((0, 64),))
    gain = jnp.clip(1.0 + 0.18 * jax.random.normal(key_of[1], (D,), jnp.float32), 0.1, 1.9)
    gate_weight = gaussian(key_of[2], (D, FF), D ** -0.5, 0.125, ((0, 32), (1, 8)))
    up_weight = gaussian(key_of[3], (D, FF), D ** -0.5, 0.125, ((0, 32), (1, 8)))
    down_weight = gaussian(key_of[4], (D, FF), FF ** -0.5, 0.109375, ((0, 32), (1, 8)))
    cotangent = bell_draw_with(key_of[5], (TOKENS, D), 1.0, 16.0, ((0, 64),), (0, 1, 64, 4.0))
    return {"inputs": inputs, "gain": gain, "gate_weight": gate_weight, "up_weight": up_weight, "down_weight": down_weight, "cotangent": cotangent}


EPS = 1e-06

def reference(inputs, gain, gate_weight, up_weight, down_weight, cotangent):
    single_precision = inputs.astype(jnp.float32)
    reciprocal_root_mean = lax.rsqrt(lax.optimization_barrier(jnp.mean(single_precision * single_precision, axis=-1, keepdims=True)) + EPS)
    unit_input = single_precision * reciprocal_root_mean
    normalized_input = (unit_input * gain).astype(jnp.bfloat16)
    gate = jnp.dot(normalized_input, gate_weight, preferred_element_type=jnp.float32)
    up_proj = jnp.dot(normalized_input, up_weight, preferred_element_type=jnp.float32)
    gate_sig = jax.nn.sigmoid(gate)
    active = gate * gate_sig
    hidden = (active * up_proj).astype(jnp.bfloat16)
    d_hidden = 0.5 * lax.dot_general(cotangent, down_weight, (((1,), (0,)), ((), ())), preferred_element_type=jnp.float32)
    d_down = 0.5 * lax.dot_general(cotangent, hidden, (((0,), (0,)), ((), ())), preferred_element_type=jnp.float32)
    d_gate = (d_hidden * up_proj * gate_sig * (1.0 + gate * (1.0 - gate_sig))).astype(jnp.bfloat16)
    d_up = (d_hidden * active).astype(jnp.bfloat16)
    unit_width = FF // N_TP
    normalized_gradient = jnp.zeros(single_precision.shape, jnp.float32)
    for column_block in range(N_TP):
        first = column_block * unit_width
        partial_value = lax.dot_general(d_gate[:, first:first + unit_width], gate_weight[:, first:first + unit_width], (((1,), (1,)), ((), ())), preferred_element_type=jnp.float32)
        partial_value = partial_value + lax.dot_general(d_up[:, first:first + unit_width], up_weight[:, first:first + unit_width], (((1,), (1,)), ((), ())), preferred_element_type=jnp.float32)
        rounded = lax.optimization_barrier(partial_value.astype(jnp.bfloat16))
        normalized_gradient = normalized_gradient + rounded.astype(jnp.float32)
    summed_rounded = lax.optimization_barrier(normalized_gradient.astype(jnp.bfloat16))
    normalized_gradient = summed_rounded.astype(jnp.float32)
    gain_gradient = lax.optimization_barrier(jnp.sum(normalized_gradient * unit_input, axis=0))
    gain_scaled = gain * normalized_gradient
    mean_correction = lax.optimization_barrier(jnp.mean(gain_scaled * unit_input, axis=-1, keepdims=True))
    input_gradient = (cotangent.astype(jnp.float32) + reciprocal_root_mean * (gain_scaled - unit_input * mean_correction)).astype(jnp.bfloat16)
    return (input_gradient, gain_gradient, d_down)
```

```python
import functools

import jax
import jax.numpy as jnp
from jax import lax
from jax.experimental import pallas as pl
from jax.experimental.pallas import tpu as pltpu
from jax.sharding import Mesh
from jax.sharding import PartitionSpec as P

FS = ("fs_0", "fs_1")
REP_FS = ("rep", "fs_0", "fs_1")
TP = ("x", "c")
RING = ("rep", "fs_0")
PLANE = ("fs_1", "x", "c")
EPS = 1e-06
F32 = jnp.float32
BF16 = jnp.bfloat16


def shifted(v, axis, by):
    n = lax.axis_size(axis)
    return lax.ppermute(v, axis, [(i, (i + by) % n) for i in range(n)])


def exchanged(v, axis):
    return lax.all_to_all(v, axis, 0, 0, tiled=True)


def from_all(v, axis):
    n = lax.axis_size(axis)
    return exchanged(jnp.broadcast_to(v[None], (n, *v.shape)), axis)


def rolled(v, start):
    return lax.dynamic_slice_in_dim(jnp.concatenate([v, v], axis=0), start, v.shape[0], axis=0)


def blocks_of(refs):
    for d in range(4):
        yield d, 0, refs[d]
    yield 4, 0, refs[4]
    yield 4, refs[4].shape[0], refs[5]
    for d in range(5, 8):
        yield d, 0, refs[d + 1]


def grad_kernel(x_ref, c_ref, *refs):
    w_refs, (mine_ref, other_ref, hid_ref) = refs[:9], refs[9:]
    units = hid_ref.shape[1]
    half = mine_ref.shape[1]
    gu = dh = None
    for d, lo, w in blocks_of(w_refs):
        rows = w.shape[0]
        a = jnp.dot(x_ref[d, :, lo : lo + rows], w[:, : 2 * units], preferred_element_type=F32)
        b = jnp.dot(c_ref[d, :, lo : lo + rows], w[:, 2 * units :], preferred_element_type=F32)
        gu = a if gu is None else gu + a
        dh = b if dh is None else dh + b
    gate, up = gu[:, :units], gu[:, units:]
    dh = 0.5 * dh
    sig = jax.nn.sigmoid(gate)
    act = gate * sig
    hid_ref[...] = (act * up).astype(BF16)
    d_gate = (dh * up * sig * (1.0 + gate * (1.0 - sig))).astype(BF16)
    d_up = (dh * act).astype(BF16)
    both = jnp.concatenate([d_gate, d_up], axis=1)
    for d, lo, w in blocks_of(w_refs):
        rows = w.shape[0]
        out = lax.dot_general(
            both, w[:, : 2 * units], (((1,), (1,)), ((), ())), preferred_element_type=F32
        ).astype(BF16)
        mine_ref[d, :, lo : lo + rows] = out[:half]
        other_ref[d, :, lo : lo + rows] = out[half:]


def down_kernel(ct_ref, hid_ref, out_ref):
    ny, nz, rows, _ = out_ref.shape
    for d in range(nz):
        res = jnp.dot(ct_ref[d], hid_ref[...], preferred_element_type=F32)
        res = (0.5 * res).astype(BF16)
        for y in range(ny):
            out_ref[y, d] = res[y * rows : (y + 1) * rows]


def vmem(n):
    return [pl.BlockSpec(memory_space=pltpu.VMEM)] * n


def local(inputs, gain, gate_weight, up_weight, down_weight, cotangent):
    nz, ny, nx = lax.axis_size("fs_0"), lax.axis_size("fs_1"), lax.axis_size("x")
    rep, zl = lax.axis_index("rep"), lax.axis_index("fs_0")
    x, c = lax.axis_index("x"), lax.axis_index("c")
    tokens, width = inputs.shape
    rows, units = gate_weight.shape
    cols = width // nz
    half, part = tokens // 2, tokens // 2 // nx

    w = jnp.concatenate([gate_weight, up_weight, down_weight], axis=1)
    w0 = from_all(w, "fs_1").reshape(ny * rows, 3 * units)
    fwd, bwd = [w0], [w0]
    for k in range(3):
        fwd.append(shifted(fwd[-1], RING, 1))
        bwd.append(shifted(bwd[-1], RING, -1))
    mid = cols // 2
    last_f = shifted(fwd[-1][:mid], RING, 1)
    last_b = shifted(bwd[-1][mid:], RING, -1)
    weights = [w0, bwd[1], bwd[2], bwd[3], last_f, last_b, fwd[3], fwd[2], fwd[1]]

    x32 = inputs.astype(F32)
    inv = lax.rsqrt(jnp.mean(x32 * x32, axis=-1, keepdims=True) + EPS)
    normed = (x32 * inv * gain).astype(BF16)

    def arranged(v):
        v = rolled(v.reshape(2, half, width), c).reshape(tokens, nz, cols)
        return rolled(v.transpose(1, 0, 2), zl)

    xr = arranged(normed)
    cr = arranged(cotangent)
    ct = cr.transpose(0, 2, 1)

    mine, other, hidden = pl.pallas_call(
        grad_kernel,
        out_shape=(
            jax.ShapeDtypeStruct((nz, half, cols), BF16),
            jax.ShapeDtypeStruct((nz, half, cols), BF16),
            jax.ShapeDtypeStruct((tokens, units), BF16),
        ),
        in_specs=vmem(11),
        out_specs=tuple(vmem(3)),
        name="grad",
    )(xr, cr, *weights)
    (dd,) = pl.pallas_call(
        down_kernel,
        out_shape=(jax.ShapeDtypeStruct((ny, nz, rows, units), BF16),),
        in_specs=vmem(2),
        out_specs=tuple(vmem(1)),
        name="down",
    )(ct, hidden)

    theirs = shifted(other, "c", 1)
    chip = (mine.astype(F32) + theirs.astype(F32)).astype(BF16)
    chip = chip.reshape(nz, nx, part, cols).transpose(1, 0, 2, 3)
    got = exchanged(chip, "x").astype(F32)
    dn = (got[0] + got[1] + got[2] + got[3]).astype(BF16)
    dn = rolled(dn, (nz - zl) % nz).transpose(1, 0, 2).reshape(part, width).astype(F32)
    first = c * half + x * part
    xs = lax.dynamic_slice_in_dim(inputs, first, part, axis=0).astype(F32)
    cs = lax.dynamic_slice_in_dim(cotangent, first, part, axis=0).astype(F32)
    inv_s = lax.rsqrt(jnp.mean(xs * xs, axis=-1, keepdims=True) + EPS)
    xhat = xs * inv_s
    gain_part = jnp.sum(dn * xhat, axis=0)
    gs = gain * dn
    m = jnp.mean(gs * xhat, axis=-1, keepdims=True)
    ig = (cs + inv_s * (gs - xhat * m)).astype(BF16)
    ig_mine = from_all(ig, "x").reshape(half, width)
    ig_other = shifted(ig_mine, "c", 1)
    out = lax.dynamic_update_slice_in_dim(jnp.zeros((tokens, width), BF16), ig_mine, c * half, 0)
    out = lax.dynamic_update_slice_in_dim(out, ig_other, (1 - c) * half, 0)

    gain_plane = jnp.sum(from_all(gain_part, PLANE), axis=0)
    gain_gradient = jnp.sum(from_all(gain_plane, RING), axis=0)

    dy = jnp.sum(exchanged(dd, "fs_1").astype(F32), axis=0).astype(BF16)
    dz = rolled(dy, (nz - zl) % nz).reshape(nz, 2, rows // 2, units).transpose(1, 0, 2, 3)
    dz = exchanged(dz.reshape(2 * nz, rows // 2, units), RING)
    own = jnp.sum(dz.astype(F32), axis=0)
    far = shifted(own, "rep", 1)
    pair = rolled(jnp.stack([own, far]), rep)
    d_down = pair.reshape(rows, units)
    return (out, gain_gradient, d_down)


def solution(mesh):
    torus = Mesh(
        mesh.devices.reshape(mesh.shape["rep"], 8, 4, 4, 2),
        ("rep", "fs_0", "fs_1", "x", "c"),
    )
    return jax.shard_map(
        local,
        mesh=torus,
        in_specs=(P(REP_FS, None), P(), P(FS, TP), P(FS, TP), P(FS, TP), P(REP_FS, None)),
        out_specs=(P(REP_FS, None), P(), P(FS, TP)),
        check_vma=False,
    )
```

```python
import jax
import jax.numpy as jnp
from jax import lax
from jax.experimental import pallas as pl
from jax.experimental.pallas import tpu as pltpu
from jax.sharding import Mesh
from jax.sharding import PartitionSpec as P

FS = ("fs_0", "fs_1")
REP_FS = ("rep", "fs_0", "fs_1")
TP = ("x", "c")
RING = ("rep", "fs_0")
PLANE = ("fs_1", "x", "c")
EPS = 1e-06
F32 = jnp.float32
BF16 = jnp.bfloat16


def shifted(v, axis, by):
    n = lax.axis_size(axis)
    return lax.ppermute(v, axis, [(i, (i + by) % n) for i in range(n)])


def exchanged(v, axis):
    return lax.all_to_all(v, axis, 0, 0, tiled=True)


def from_all(v, axis):
    n = lax.axis_size(axis)
    return exchanged(jnp.broadcast_to(v[None], (n, *v.shape)), axis)


def rolled(v, start):
    return lax.dynamic_slice_in_dim(jnp.concatenate([v, v], axis=0), start, v.shape[0], axis=0)


def blocks_of(refs):
    for d in range(4):
        yield d, 0, refs[d]
    yield 4, 0, refs[4]
    yield 4, refs[4].shape[0], refs[5]
    for d in range(5, 8):
        yield d, 0, refs[d + 1]


def prepare_tokens(at_ref, x_ref, gain_ref, out_ref):
    nz, _, cols = out_ref.shape
    v = x_ref[...].astype(F32)
    inv = lax.rsqrt(jnp.mean(v * v, axis=-1, keepdims=True) + EPS)
    for d in range(nz):
        own = pl.ds(pl.multiple_of(((at_ref[0] + d) % nz) * cols, cols), cols)
        part = x_ref[:, own].astype(F32)
        out_ref[d] = (part * inv * gain_ref[:, own]).astype(BF16)


def prepare_cotangent(at_ref, lo_ref, hi_ref, out_ref, turned_ref):
    nz, _, cols = out_ref.shape
    for d in range(nz):
        own = pl.ds(pl.multiple_of(((at_ref[0] + d) % nz) * cols, cols), cols)
        part = jnp.concatenate([lo_ref[:, own], hi_ref[:, own]], axis=0)
        out_ref[d] = part
        turned_ref[d] = part.T


def grad_kernel(x_ref, c_ref, *refs):
    w_refs, (mine_ref, other_ref, hid_ref) = refs[:9], refs[9:]
    units = hid_ref.shape[1]
    nx, _, part, _ = mine_ref.shape
    gu = dh = None
    for d, lo, w in blocks_of(w_refs):
        rows = w.shape[0]
        a = jnp.dot(x_ref[d, :, lo : lo + rows], w[:, : 2 * units], preferred_element_type=F32)
        b = jnp.dot(c_ref[d, :, lo : lo + rows], w[:, 2 * units :], preferred_element_type=F32)
        gu = a if gu is None else gu + a
        dh = b if dh is None else dh + b
    gate, up = gu[:, :units], gu[:, units:]
    dh = 0.5 * dh
    sig = jax.nn.sigmoid(gate)
    act = gate * sig
    hid_ref[...] = (act * up).astype(BF16)
    d_gate = (dh * up * sig * (1.0 + gate * (1.0 - sig))).astype(BF16)
    d_up = (dh * act).astype(BF16)
    both = jnp.concatenate([d_gate, d_up], axis=1)
    for d, lo, w in blocks_of(w_refs):
        rows = w.shape[0]
        out = lax.dot_general(
            both, w[:, : 2 * units], (((1,), (1,)), ((), ())), preferred_element_type=F32
        ).astype(BF16)
        for k in range(nx):
            mine_ref[k, d, :, lo : lo + rows] = out[k * part : (k + 1) * part]
            other_ref[k, d, :, lo : lo + rows] = out[(nx + k) * part : (nx + k + 1) * part]


def down_kernel(ct_ref, hid_ref, out_ref):
    ny, nz, rows, _ = out_ref.shape
    for d in range(nz):
        res = jnp.dot(ct_ref[d], hid_ref[...], preferred_element_type=F32)
        res = (0.5 * res).astype(BF16)
        for y in range(ny):
            out_ref[y, d] = res[y * rows : (y + 1) * rows]


def chip_kernel(mine_ref, theirs_ref, *out_refs):
    for k, out_ref in enumerate(out_refs):
        out_ref[...] = (mine_ref[k].astype(F32) + theirs_ref[k].astype(F32)).astype(BF16)


def finish_kernel(at_ref, got0, got1, got2, got3, x_ref, c_ref, gain_ref, out_ref, sum_ref, dn_ref):
    nz, _, cols = got0.shape
    for d in range(nz):
        own = pl.ds(pl.multiple_of(((at_ref[0] + d) % nz) * cols, cols), cols)
        total = got0[d].astype(F32)
        for got in (got1, got2, got3):
            total = total + got[d].astype(F32)
        dn_ref[:, own] = total.astype(BF16)
    v = x_ref[...].astype(F32)
    inv = lax.rsqrt(jnp.mean(v * v, axis=-1, keepdims=True) + EPS)
    xhat = v * inv
    dn = dn_ref[...].astype(F32)
    sums = jnp.sum(dn * xhat, axis=0, keepdims=True)
    gs = gain_ref[...] * dn
    m = jnp.mean(gs * xhat, axis=-1, keepdims=True)
    out_ref[...] = (c_ref[...].astype(F32) + inv * (gs - xhat * m)).astype(BF16)
    for k in range(sum_ref.shape[0]):
        sum_ref[k] = sums


def place_kernel(at_ref, p0, p1, p2, p3, other_ref, out_ref):
    n = 4
    part = p0.shape[0]
    for k, piece in enumerate((p0, p1, p2, p3)):
        spot = (at_ref[2] + k) % n
        own = pl.multiple_of((at_ref[1] * n + spot) * part, part)
        out_ref[pl.ds(own, part), :] = piece[...]
        far = pl.multiple_of(((1 - at_ref[1]) * n + spot) * part, part)
        out_ref[pl.ds(far, part), :] = other_ref[k]


def vmem(n):
    return [pl.BlockSpec(memory_space=pltpu.VMEM)] * n


def work(inputs, gain, gate_weight, up_weight, down_weight, cotangent):
    nz, ny, nx = lax.axis_size("fs_0"), lax.axis_size("fs_1"), lax.axis_size("x")
    rep, zl = lax.axis_index("rep"), lax.axis_index("fs_0")
    x, c = lax.axis_index("x"), lax.axis_index("c")
    tokens, width = inputs.shape
    rows, units = gate_weight.shape
    cols = width // nz
    half, part = tokens // 2, tokens // 2 // nx
    gain2 = gain[None]
    at = jnp.stack([zl, c, x]).astype(jnp.int32)

    w = jnp.concatenate([gate_weight, up_weight, down_weight], axis=1)
    w0 = from_all(w, "fs_1").reshape(ny * rows, 3 * units)
    fwd, bwd = [w0], [w0]
    for _ in range(3):
        fwd.append(shifted(fwd[-1], RING, 1))
        bwd.append(shifted(bwd[-1], RING, -1))
    mid = cols // 2
    last_f = shifted(fwd[-1][:mid], RING, 1)
    last_b = shifted(bwd[-1][mid:], RING, -1)
    weights = [w0, bwd[1], bwd[2], bwd[3], last_f, last_b, fwd[3], fwd[2], fwd[1]]

    def spot(i, at):
        return ((i // nx + at[1]) % 2) * nx + (i + at[2]) % nx

    xr = pl.pallas_call(
        prepare_tokens,
        out_shape=jax.ShapeDtypeStruct((nz, tokens, cols), BF16),
        grid_spec=pltpu.PrefetchScalarGridSpec(
            num_scalar_prefetch=1,
            grid=(2 * nx,),
            in_specs=[
                pl.BlockSpec((part, width), lambda i, at: (spot(i, at), 0)),
                pl.BlockSpec((1, width), lambda i, at: (0, 0)),
            ],
            out_specs=pl.BlockSpec((nz, part, cols), lambda i, at: (0, i, 0)),
        ),
        name="prepare_x",
    )(at, inputs, gain2)
    cr, ct = pl.pallas_call(
        prepare_cotangent,
        out_shape=(
            jax.ShapeDtypeStruct((nz, tokens, cols), BF16),
            jax.ShapeDtypeStruct((nz, cols, tokens), BF16),
        ),
        grid_spec=pltpu.PrefetchScalarGridSpec(
            num_scalar_prefetch=1,
            grid=(nx,),
            in_specs=[
                pl.BlockSpec((part, width), lambda i, at: (spot(2 * i, at), 0)),
                pl.BlockSpec((part, width), lambda i, at: (spot(2 * i + 1, at), 0)),
            ],
            out_specs=(
                pl.BlockSpec((nz, 2 * part, cols), lambda i, at: (0, i, 0)),
                pl.BlockSpec((nz, cols, 2 * part), lambda i, at: (0, 0, i)),
            ),
        ),
        name="prepare_c",
    )(at, cotangent, cotangent)

    mine, other, hidden = pl.pallas_call(
        grad_kernel,
        out_shape=(
            jax.ShapeDtypeStruct((nx, nz, part, cols), BF16),
            jax.ShapeDtypeStruct((nx, nz, part, cols), BF16),
            jax.ShapeDtypeStruct((tokens, units), BF16),
        ),
        in_specs=vmem(11),
        out_specs=tuple(vmem(3)),
        name="grad",
    )(xr, cr, *weights)
    theirs = shifted(other, "c", 1)
    (dd,) = pl.pallas_call(
        down_kernel,
        out_shape=(jax.ShapeDtypeStruct((ny, nz, rows, units), BF16),),
        in_specs=vmem(2),
        out_specs=tuple(vmem(1)),
        name="down",
    )(ct, hidden)
    dy = exchanged(dd, "fs_1")

    chunk = jax.ShapeDtypeStruct((nz, part, cols), BF16)
    chip = pl.pallas_call(
        chip_kernel,
        out_shape=(chunk,) * 4,
        in_specs=vmem(2),
        out_specs=tuple(vmem(4)),
        name="chip",
    )(mine, theirs)
    got = [chip[0]]
    for k in (1, 2, 3):
        got.append(shifted(chip[k], "x", k))
    first = c * half + x * part
    xs = lax.dynamic_slice_in_dim(inputs, first, part, axis=0)
    cs = lax.dynamic_slice_in_dim(cotangent, first, part, axis=0)
    planes = lax.axis_size(PLANE)
    ig, gain_part = pl.pallas_call(
        finish_kernel,
        out_shape=(
            jax.ShapeDtypeStruct((part, width), BF16),
            jax.ShapeDtypeStruct((planes, 1, width), F32),
        ),
        in_specs=[pl.BlockSpec(memory_space=pltpu.SMEM)] + vmem(7),
        out_specs=tuple(vmem(2)),
        scratch_shapes=[pltpu.VMEM((part, width), BF16)],
        name="finish",
    )(at, *got, xs, cs, gain2)
    pieces = [ig]
    for k in (1, 2, 3):
        pieces.append(shifted(ig, "x", -k))
    ig_other = shifted(jnp.stack(pieces), "c", 1)
    out = pl.pallas_call(
        place_kernel,
        out_shape=jax.ShapeDtypeStruct((tokens, width), BF16),
        in_specs=[pl.BlockSpec(memory_space=pltpu.SMEM)] + vmem(5),
        out_specs=pl.BlockSpec(memory_space=pltpu.VMEM),
        name="place",
    )(at, *pieces, ig_other)

    gain_plane = exchanged(gain_part, PLANE)
    gain_plane = jnp.sum(gain_plane, axis=0)
    gain_gradient = from_all(gain_plane, RING)
    gain_gradient = jnp.sum(gain_gradient, axis=(0, 1))

    dy = jnp.sum(dy.astype(F32), axis=0).astype(BF16)
    dz = rolled(dy, (nz - zl) % nz).reshape(nz, 2, rows // 2, units).transpose(1, 0, 2, 3)
    dz = exchanged(dz.reshape(2 * nz, rows // 2, units), RING)
    own = jnp.sum(dz.astype(F32), axis=0)
    far = shifted(own, "rep", 1)
    pair = rolled(jnp.stack([own, far]), rep)
    d_down = pair.reshape(rows, units)
    return (out, gain_gradient, d_down)


def solution(mesh):
    torus = Mesh(
        mesh.devices.reshape(mesh.shape["rep"], 8, 4, 4, 2),
        ("rep", "fs_0", "fs_1", "x", "c"),
    )
    return jax.shard_map(
        work,
        mesh=torus,
        in_specs=(P(REP_FS, None), P(), P(FS, TP), P(FS, TP), P(FS, TP), P(REP_FS, None)),
        out_specs=(P(REP_FS, None), P(), P(FS, TP)),
        check_vma=False,
    )
```

```python
import jax
import jax.numpy as jnp
from jax import lax
from jax.experimental import pallas as pl
from jax.experimental.pallas import tpu as pltpu
from jax.sharding import Mesh
from jax.sharding import PartitionSpec as P

FS = ("fs_0", "fs_1")
REP_FS = ("rep", "fs_0", "fs_1")
TP = ("x", "c")
RING = ("rep", "fs_0")
PLANE = ("fs_1", "x", "c")
EPS = 1e-06
F32 = jnp.float32
BF16 = jnp.bfloat16


def shifted(v, axis, by):
    n = lax.axis_size(axis)
    return lax.ppermute(v, axis, [(i, (i + by) % n) for i in range(n)])


def exchanged(v, axis):
    return lax.all_to_all(v, axis, 0, 0, tiled=True)


def from_all(v, axis):
    n = lax.axis_size(axis)
    return exchanged(jnp.broadcast_to(v[None], (n, *v.shape)), axis)


def rolled(v, start):
    return lax.dynamic_slice_in_dim(jnp.concatenate([v, v], axis=0), start, v.shape[0], axis=0)


def blocks_of(refs):
    for d in range(4):
        yield d, 0, refs[d]
    yield 4, 0, refs[4]
    yield 4, refs[4].shape[0], refs[5]
    for d in range(5, 8):
        yield d, 0, refs[d + 1]


def prepare_tokens(at_ref, x_ref, gain_ref, out_ref):
    nz, _, cols = out_ref.shape
    v = x_ref[...].astype(F32)
    inv = lax.rsqrt(jnp.mean(v * v, axis=-1, keepdims=True) + EPS)
    for d in range(nz):
        own = pl.ds(pl.multiple_of(((at_ref[0] + d) % nz) * cols, cols), cols)
        part = x_ref[:, own].astype(F32)
        out_ref[d] = (part * inv * gain_ref[:, own]).astype(BF16)


def prepare_cotangent(at_ref, lo_ref, hi_ref, out_ref, turned_ref):
    nz, _, cols = out_ref.shape
    for d in range(nz):
        own = pl.ds(pl.multiple_of(((at_ref[0] + d) % nz) * cols, cols), cols)
        part = jnp.concatenate([lo_ref[:, own], hi_ref[:, own]], axis=0)
        out_ref[d] = part
        turned_ref[d] = part.T


def grad_kernel(x_ref, c_ref, *refs):
    w_refs, (mine_ref, other_ref, hid_ref) = refs[:9], refs[9:]
    units = hid_ref.shape[1]
    nx, _, part, _ = mine_ref.shape
    gu = dh = None
    for d, lo, w in blocks_of(w_refs):
        rows = w.shape[0]
        a = jnp.dot(x_ref[d, :, lo : lo + rows], w[:, : 2 * units], preferred_element_type=F32)
        b = jnp.dot(c_ref[d, :, lo : lo + rows], w[:, 2 * units :], preferred_element_type=F32)
        gu = a if gu is None else gu + a
        dh = b if dh is None else dh + b
    gate, up = gu[:, :units], gu[:, units:]
    dh = 0.5 * dh
    sig = jax.nn.sigmoid(gate)
    act = gate * sig
    hid_ref[...] = (act * up).astype(BF16)
    d_gate = (dh * up * sig * (1.0 + gate * (1.0 - sig))).astype(BF16)
    d_up = (dh * act).astype(BF16)
    both = jnp.concatenate([d_gate, d_up], axis=1)
    for d, lo, w in blocks_of(w_refs):
        rows = w.shape[0]
        out = lax.dot_general(
            both, w[:, : 2 * units], (((1,), (1,)), ((), ())), preferred_element_type=F32
        ).astype(BF16)
        for k in range(nx):
            mine_ref[k, d, :, lo : lo + rows] = out[k * part : (k + 1) * part]
            other_ref[k, d, :, lo : lo + rows] = out[(nx + k) * part : (nx + k + 1) * part]


def down_kernel(ct_ref, hid_ref, out_ref):
    ny, nz, rows, _ = out_ref.shape
    for d in range(nz):
        res = jnp.dot(ct_ref[d], hid_ref[...], preferred_element_type=F32)
        res = (0.5 * res).astype(BF16)
        for y in range(ny):
            out_ref[y, d] = res[y * rows : (y + 1) * rows]


def chip_kernel(mine_ref, theirs_ref, *out_refs):
    for k, out_ref in enumerate(out_refs):
        out_ref[...] = (mine_ref[k].astype(F32) + theirs_ref[k].astype(F32)).astype(BF16)


def finish_kernel(at_ref, got0, got1, got2, got3, x_ref, c_ref, gain_ref, out_ref, sum_ref, dn_ref):
    nz, _, cols = got0.shape
    for d in range(nz):
        own = pl.ds(pl.multiple_of(((at_ref[0] + d) % nz) * cols, cols), cols)
        total = got0[d].astype(F32)
        for got in (got1, got2, got3):
            total = total + got[d].astype(F32)
        dn_ref[:, own] = total.astype(BF16)
    v = x_ref[...].astype(F32)
    inv = lax.rsqrt(jnp.mean(v * v, axis=-1, keepdims=True) + EPS)
    xhat = v * inv
    dn = dn_ref[...].astype(F32)
    sums = jnp.sum(dn * xhat, axis=0, keepdims=True)
    gs = gain_ref[...] * dn
    m = jnp.mean(gs * xhat, axis=-1, keepdims=True)
    out_ref[...] = (c_ref[...].astype(F32) + inv * (gs - xhat * m)).astype(BF16)
    for k in range(sum_ref.shape[0]):
        sum_ref[k] = sums


def place_kernel(at_ref, p0, p1, p2, p3, other_ref, out_ref, sems):
    n = 4
    part = p0.shape[0]
    copies = []
    for k, piece in enumerate((p0, p1, p2, p3)):
        spot = (at_ref[2] + k) % n
        own = pl.multiple_of((at_ref[1] * n + spot) * part, part)
        far = pl.multiple_of(((1 - at_ref[1]) * n + spot) * part, part)
        copies.append(
            pltpu.make_async_copy(piece, out_ref.at[pl.ds(own, part), :], sems.at[2 * k])
        )
        copies.append(
            pltpu.make_async_copy(
                other_ref.at[k], out_ref.at[pl.ds(far, part), :], sems.at[2 * k + 1]
            )
        )
    for copy in copies:
        copy.start()
    for copy in copies:
        copy.wait()


def rows_kernel(at_ref, got_ref, out_ref):
    ny, nz, rows, _ = got_ref.shape
    half = rows // 2
    for d in range(nz):
        total = got_ref[0, d].astype(F32)
        for k in range(1, ny):
            total = total + got_ref[k, d].astype(F32)
        total = total.astype(BF16)
        to = (at_ref[0] + d) % nz
        out_ref[to] = total[:half]
        out_ref[nz + to] = total[half:]


def ring_kernel(got_ref, out_ref):
    total = got_ref[0].astype(F32)
    for k in range(1, got_ref.shape[0]):
        total = total + got_ref[k].astype(F32)
    out_ref[...] = total


def vmem(n):
    return [pl.BlockSpec(memory_space=pltpu.VMEM)] * n


def work(inputs, gain, gate_weight, up_weight, down_weight, cotangent):
    nz, ny, nx = lax.axis_size("fs_0"), lax.axis_size("fs_1"), lax.axis_size("x")
    rep, zl = lax.axis_index("rep"), lax.axis_index("fs_0")
    x, c = lax.axis_index("x"), lax.axis_index("c")
    tokens, width = inputs.shape
    rows, units = gate_weight.shape
    cols = width // nz
    part = tokens // 2 // nx
    gain2 = gain[None]
    at = jnp.stack([zl, c, x]).astype(jnp.int32)

    w = jnp.concatenate([gate_weight, up_weight, down_weight], axis=1)
    w0 = from_all(w, "fs_1").reshape(ny * rows, 3 * units)
    fwd, bwd = [w0], [w0]
    for _ in range(3):
        fwd.append(shifted(fwd[-1], RING, 1))
        bwd.append(shifted(bwd[-1], RING, -1))
    mid = cols // 2
    last_f = shifted(fwd[-1][:mid], RING, 1)
    last_b = shifted(bwd[-1][mid:], RING, -1)
    weights = [w0, bwd[1], bwd[2], bwd[3], last_f, last_b, fwd[3], fwd[2], fwd[1]]

    def spot(i, at):
        return ((i // nx + at[1]) % 2) * nx + (i + at[2]) % nx

    xr = pl.pallas_call(
        prepare_tokens,
        out_shape=jax.ShapeDtypeStruct((nz, tokens, cols), BF16),
        grid_spec=pltpu.PrefetchScalarGridSpec(
            num_scalar_prefetch=1,
            grid=(2 * nx,),
            in_specs=[
                pl.BlockSpec((part, width), lambda i, at: (spot(i, at), 0)),
                pl.BlockSpec((1, width), lambda i, at: (0, 0)),
            ],
            out_specs=pl.BlockSpec((nz, part, cols), lambda i, at: (0, i, 0)),
        ),
        name="prepare_x",
    )(at, inputs, gain2)
    cr, ct = pl.pallas_call(
        prepare_cotangent,
        out_shape=(
            jax.ShapeDtypeStruct((nz, tokens, cols), BF16),
            jax.ShapeDtypeStruct((nz, cols, tokens), BF16),
        ),
        grid_spec=pltpu.PrefetchScalarGridSpec(
            num_scalar_prefetch=1,
            grid=(nx,),
            in_specs=[
                pl.BlockSpec((part, width), lambda i, at: (spot(2 * i, at), 0)),
                pl.BlockSpec((part, width), lambda i, at: (spot(2 * i + 1, at), 0)),
            ],
            out_specs=(
                pl.BlockSpec((nz, 2 * part, cols), lambda i, at: (0, i, 0)),
                pl.BlockSpec((nz, cols, 2 * part), lambda i, at: (0, 0, i)),
            ),
        ),
        name="prepare_c",
    )(at, cotangent, cotangent)

    mine, other, hidden = pl.pallas_call(
        grad_kernel,
        out_shape=(
            jax.ShapeDtypeStruct((nx, nz, part, cols), BF16),
            jax.ShapeDtypeStruct((nx, nz, part, cols), BF16),
            jax.ShapeDtypeStruct((tokens, units), BF16),
        ),
        in_specs=vmem(11),
        out_specs=tuple(vmem(3)),
        name="grad",
    )(xr, cr, *weights)
    theirs = shifted(other, "c", 1)
    (dd,) = pl.pallas_call(
        down_kernel,
        out_shape=(jax.ShapeDtypeStruct((ny, nz, rows, units), BF16),),
        in_specs=vmem(2),
        out_specs=tuple(vmem(1)),
        name="down",
    )(ct, hidden)
    dy = exchanged(dd, "fs_1")

    chunk = jax.ShapeDtypeStruct((nz, part, cols), BF16)
    chip = pl.pallas_call(
        chip_kernel,
        out_shape=(chunk,) * 4,
        in_specs=vmem(2),
        out_specs=tuple(vmem(4)),
        name="chip",
    )(mine, theirs)
    got = [chip[0]]
    for k in (1, 2, 3):
        got.append(shifted(chip[k], "x", k))
    planes = lax.axis_size(PLANE)
    whole = pl.BlockSpec((nz, part, cols), lambda i, at: (0, 0, 0))
    own = pl.BlockSpec((part, width), lambda i, at: (at[1] * nx + at[2], 0))
    ig, gain_part = pl.pallas_call(
        finish_kernel,
        out_shape=(
            jax.ShapeDtypeStruct((part, width), BF16),
            jax.ShapeDtypeStruct((planes, 1, width), F32),
        ),
        grid_spec=pltpu.PrefetchScalarGridSpec(
            num_scalar_prefetch=1,
            grid=(1,),
            in_specs=[whole] * 4 + [own, own, pl.BlockSpec((1, width), lambda i, at: (0, 0))],
            out_specs=(
                pl.BlockSpec((part, width), lambda i, at: (0, 0)),
                pl.BlockSpec((planes, 1, width), lambda i, at: (0, 0, 0)),
            ),
            scratch_shapes=[pltpu.VMEM((part, width), BF16)],
        ),
        name="finish",
    )(at, *got, inputs, cotangent, gain2)
    pieces = [ig]
    for k in (1, 2, 3):
        pieces.append(shifted(ig, "x", -k))
    ig_other = shifted(jnp.stack(pieces), "c", 1)
    out = pl.pallas_call(
        place_kernel,
        out_shape=jax.ShapeDtypeStruct((tokens, width), BF16),
        in_specs=[pl.BlockSpec(memory_space=pltpu.SMEM)] + [pl.BlockSpec(memory_space=pl.ANY)] * 5,
        out_specs=pl.BlockSpec(memory_space=pl.ANY),
        scratch_shapes=[pltpu.SemaphoreType.DMA((8,))],
        name="place",
    )(at, *pieces, ig_other)

    gain_plane = exchanged(gain_part, PLANE)
    gain_plane = jnp.sum(gain_plane, axis=0)
    gain_gradient = from_all(gain_plane, RING)
    gain_gradient = jnp.sum(gain_gradient, axis=(0, 1))

    dz = pl.pallas_call(
        rows_kernel,
        out_shape=jax.ShapeDtypeStruct((2 * nz, rows // 2, units), BF16),
        in_specs=[pl.BlockSpec(memory_space=pltpu.SMEM)] + vmem(1),
        out_specs=pl.BlockSpec(memory_space=pltpu.VMEM),
        name="ysum",
    )(at, dy)
    dz = exchanged(dz, RING)
    own = pl.pallas_call(
        ring_kernel,
        out_shape=jax.ShapeDtypeStruct((rows // 2, units), F32),
        in_specs=vmem(1),
        out_specs=pl.BlockSpec(memory_space=pltpu.VMEM),
        name="zsum",
    )(dz)
    far = shifted(own, "rep", 1)
    pair = rolled(jnp.stack([own, far]), rep)
    d_down = pair.reshape(rows, units)
    return (out, gain_gradient, d_down)


def solution(mesh):
    torus = Mesh(
        mesh.devices.reshape(mesh.shape["rep"], 8, 4, 4, 2),
        ("rep", "fs_0", "fs_1", "x", "c"),
    )
    return jax.shard_map(
        work,
        mesh=torus,
        in_specs=(P(REP_FS, None), P(), P(FS, TP), P(FS, TP), P(FS, TP), P(REP_FS, None)),
        out_specs=(P(REP_FS, None), P(), P(FS, TP)),
        check_vma=False,
    )
```

```python
import jax
import jax.numpy as jnp
from jax import lax
from jax.experimental import pallas as pl
from jax.experimental.pallas import tpu as pltpu
from jax.sharding import Mesh
from jax.sharding import PartitionSpec as P

FS = ("fs_0", "fs_1")
REP_FS = ("rep", "fs_0", "fs_1")
TP = ("x", "c")
RING = ("rep", "fs_0")
EPS = 1e-06
F32 = jnp.float32
BF16 = jnp.bfloat16


def shifted(v, axis, by):
    n = lax.axis_size(axis)
    return lax.ppermute(v, axis, [(i, (i + by) % n) for i in range(n)])


def exchanged(v, axis):
    return lax.all_to_all(v, axis, 0, 0, tiled=True)


def from_all(v, axis):
    n = lax.axis_size(axis)
    return exchanged(jnp.broadcast_to(v[None], (n, *v.shape)), axis)


def rolled(v, start):
    return lax.dynamic_slice_in_dim(jnp.concatenate([v, v], axis=0), start, v.shape[0], axis=0)


def blocks_of(refs):
    for d in range(4):
        yield d, 0, refs[d]
    yield 4, 0, refs[4]
    yield 4, refs[4].shape[0], refs[5]
    for d in range(5, 8):
        yield d, 0, refs[d + 1]


def prepare_tokens(at_ref, x_ref, gain_ref, out_ref):
    nz, _, cols = out_ref.shape
    v = x_ref[...].astype(F32)
    inv = lax.rsqrt(jnp.mean(v * v, axis=-1, keepdims=True) + EPS)
    for d in range(nz):
        own = pl.ds(pl.multiple_of(((at_ref[0] + d) % nz) * cols, cols), cols)
        part = x_ref[:, own].astype(F32)
        out_ref[d] = (part * inv * gain_ref[:, own]).astype(BF16)


def prepare_cotangent(at_ref, lo_ref, hi_ref, out_ref, turned_ref):
    nz, _, cols = out_ref.shape
    for d in range(nz):
        own = pl.ds(pl.multiple_of(((at_ref[0] + d) % nz) * cols, cols), cols)
        part = jnp.concatenate([lo_ref[:, own], hi_ref[:, own]], axis=0)
        out_ref[d] = part
        turned_ref[d] = part.T


def grad_kernel(x_ref, c_ref, *refs):
    w_refs, (mine_ref, other_ref, hid_ref) = refs[:9], refs[9:]
    units = hid_ref.shape[1]
    nx, _, part, _ = mine_ref.shape
    gu = dh = None
    for d, lo, w in blocks_of(w_refs):
        rows = w.shape[0]
        a = jnp.dot(x_ref[d, :, lo : lo + rows], w[:, : 2 * units], preferred_element_type=F32)
        b = jnp.dot(c_ref[d, :, lo : lo + rows], w[:, 2 * units :], preferred_element_type=F32)
        gu = a if gu is None else gu + a
        dh = b if dh is None else dh + b
    gate, up = gu[:, :units], gu[:, units:]
    dh = 0.5 * dh
    sig = jax.nn.sigmoid(gate)
    act = gate * sig
    hid_ref[...] = (act * up).astype(BF16)
    d_gate = (dh * up * sig * (1.0 + gate * (1.0 - sig))).astype(BF16)
    d_up = (dh * act).astype(BF16)
    both = jnp.concatenate([d_gate, d_up], axis=1)
    for d, lo, w in blocks_of(w_refs):
        rows = w.shape[0]
        out = lax.dot_general(
            both, w[:, : 2 * units], (((1,), (1,)), ((), ())), preferred_element_type=F32
        ).astype(BF16)
        for k in range(nx):
            mine_ref[k, d, :, lo : lo + rows] = out[k * part : (k + 1) * part]
            other_ref[k, d, :, lo : lo + rows] = out[(nx + k) * part : (nx + k + 1) * part]


def down_kernel(ct_ref, hid_ref, out_ref):
    ny, nz, rows, _ = out_ref.shape
    for d in range(nz):
        res = jnp.dot(ct_ref[d], hid_ref[...], preferred_element_type=F32)
        res = (0.5 * res).astype(BF16)
        for y in range(ny):
            out_ref[y, d] = res[y * rows : (y + 1) * rows]


def chip_kernel(mine_ref, theirs_ref, *out_refs):
    for k, out_ref in enumerate(out_refs):
        out_ref[...] = (mine_ref[k].astype(F32) + theirs_ref[k].astype(F32)).astype(BF16)


def finish_kernel(at_ref, got0, got1, got2, got3, x_ref, c_ref, gain_ref, out_ref, dn_ref):
    nz, _, cols = got0.shape
    for d in range(nz):
        own = pl.ds(pl.multiple_of(((at_ref[0] + d) % nz) * cols, cols), cols)
        total = got0[d].astype(F32)
        for got in (got1, got2, got3):
            total = total + got[d].astype(F32)
        dn_ref[:, own] = total.astype(BF16)
    v = x_ref[...].astype(F32)
    inv = lax.rsqrt(jnp.mean(v * v, axis=-1, keepdims=True) + EPS)
    xhat = v * inv
    dn = dn_ref[...].astype(F32)
    sums = jnp.sum(dn * xhat, axis=0, keepdims=True)
    gs = gain_ref[...] * dn
    m = jnp.mean(gs * xhat, axis=-1, keepdims=True)
    part = v.shape[0]
    out_ref[:part] = (c_ref[...].astype(F32) + inv * (gs - xhat * m)).astype(BF16)
    high = sums.astype(BF16)
    left = sums - high.astype(F32)
    mid = left.astype(BF16)
    low = (left - mid.astype(F32)).astype(BF16)
    none = jnp.zeros((out_ref.shape[0] - part - 3, v.shape[1]), BF16)
    out_ref[part:] = jnp.concatenate([high, mid, low, none], axis=0)


def place_kernel(at_ref, p0, p1, p2, p3, other_ref, out_ref):
    n = 4
    part = out_ref.shape[0] // (2 * n)
    for k, piece in enumerate((p0, p1, p2, p3)):
        spot = (at_ref[2] + k) % n
        own = pl.multiple_of((at_ref[1] * n + spot) * part, part)
        far = pl.multiple_of(((1 - at_ref[1]) * n + spot) * part, part)
        out_ref[pl.ds(own, part), :] = piece[:part]
        out_ref[pl.ds(far, part), :] = other_ref[k, :part]


def gain_kernel(p0, p1, p2, p3, other_ref, out_ref):
    total = jnp.zeros(p0.shape, F32)
    for k, piece in enumerate((p0, p1, p2, p3)):
        total = total + (piece[...].astype(F32) + other_ref[k].astype(F32))
    total = jnp.sum(total, axis=0, keepdims=True)
    for k in range(out_ref.shape[0]):
        out_ref[k] = total


def vmem(n):
    return [pl.BlockSpec(memory_space=pltpu.VMEM)] * n


def work(inputs, gain, gate_weight, up_weight, down_weight, cotangent):
    nz, ny, nx = lax.axis_size("fs_0"), lax.axis_size("fs_1"), lax.axis_size("x")
    rep, zl = lax.axis_index("rep"), lax.axis_index("fs_0")
    x, c = lax.axis_index("x"), lax.axis_index("c")
    tokens, width = inputs.shape
    rows, units = gate_weight.shape
    cols = width // nz
    part = tokens // 2 // nx
    gain2 = gain[None]
    at = jnp.stack([zl, c, x]).astype(jnp.int32)

    w = jnp.concatenate([gate_weight, up_weight, down_weight], axis=1)
    w0 = from_all(w, "fs_1").reshape(ny * rows, 3 * units)
    fwd, bwd = [w0], [w0]
    for _ in range(3):
        fwd.append(shifted(fwd[-1], RING, 1))
        bwd.append(shifted(bwd[-1], RING, -1))
    mid = cols // 2
    last_f = shifted(fwd[-1][:mid], RING, 1)
    last_b = shifted(bwd[-1][mid:], RING, -1)
    weights = [w0, bwd[1], bwd[2], bwd[3], last_f, last_b, fwd[3], fwd[2], fwd[1]]

    def spot(i, at):
        return ((i // nx + at[1]) % 2) * nx + (i + at[2]) % nx

    xr = pl.pallas_call(
        prepare_tokens,
        out_shape=jax.ShapeDtypeStruct((nz, tokens, cols), BF16),
        grid_spec=pltpu.PrefetchScalarGridSpec(
            num_scalar_prefetch=1,
            grid=(2 * nx,),
            in_specs=[
                pl.BlockSpec((part, width), lambda i, at: (spot(i, at), 0)),
                pl.BlockSpec((1, width), lambda i, at: (0, 0)),
            ],
            out_specs=pl.BlockSpec((nz, part, cols), lambda i, at: (0, i, 0)),
        ),
        name="prepare_x",
    )(at, inputs, gain2)
    cr, ct = pl.pallas_call(
        prepare_cotangent,
        out_shape=(
            jax.ShapeDtypeStruct((nz, tokens, cols), BF16),
            jax.ShapeDtypeStruct((nz, cols, tokens), BF16),
        ),
        grid_spec=pltpu.PrefetchScalarGridSpec(
            num_scalar_prefetch=1,
            grid=(nx,),
            in_specs=[
                pl.BlockSpec((part, width), lambda i, at: (spot(2 * i, at), 0)),
                pl.BlockSpec((part, width), lambda i, at: (spot(2 * i + 1, at), 0)),
            ],
            out_specs=(
                pl.BlockSpec((nz, 2 * part, cols), lambda i, at: (0, i, 0)),
                pl.BlockSpec((nz, cols, 2 * part), lambda i, at: (0, 0, i)),
            ),
        ),
        name="prepare_c",
    )(at, cotangent, cotangent)

    mine, other, hidden = pl.pallas_call(
        grad_kernel,
        out_shape=(
            jax.ShapeDtypeStruct((nx, nz, part, cols), BF16),
            jax.ShapeDtypeStruct((nx, nz, part, cols), BF16),
            jax.ShapeDtypeStruct((tokens, units), BF16),
        ),
        in_specs=vmem(11),
        out_specs=tuple(vmem(3)),
        name="grad",
    )(xr, cr, *weights)
    theirs = shifted(other, "c", 1)
    (dd,) = pl.pallas_call(
        down_kernel,
        out_shape=(jax.ShapeDtypeStruct((ny, nz, rows, units), BF16),),
        in_specs=vmem(2),
        out_specs=tuple(vmem(1)),
        name="down",
    )(ct, hidden)
    dy = exchanged(dd, "fs_1")

    chunk = jax.ShapeDtypeStruct((nz, part, cols), BF16)
    chip = pl.pallas_call(
        chip_kernel,
        out_shape=(chunk,) * 4,
        in_specs=vmem(2),
        out_specs=tuple(vmem(4)),
        name="chip",
    )(mine, theirs)
    got = [chip[0]]
    for k in (1, 2, 3):
        got.append(shifted(chip[k], "x", k))
    whole = pl.BlockSpec((nz, part, cols), lambda i, at: (0, 0, 0))
    own = pl.BlockSpec((part, width), lambda i, at: (at[1] * nx + at[2], 0))
    longer = part + 8
    ig = pl.pallas_call(
        finish_kernel,
        out_shape=jax.ShapeDtypeStruct((longer, width), BF16),
        grid_spec=pltpu.PrefetchScalarGridSpec(
            num_scalar_prefetch=1,
            grid=(1,),
            in_specs=[whole] * 4 + [own, own, pl.BlockSpec((1, width), lambda i, at: (0, 0))],
            out_specs=pl.BlockSpec((longer, width), lambda i, at: (0, 0)),
            scratch_shapes=[pltpu.VMEM((part, width), BF16)],
        ),
        name="finish",
    )(at, *got, inputs, cotangent, gain2)
    pieces = [ig]
    for k in (1, 2, 3):
        pieces.append(shifted(ig, "x", -k))
    ig_other = shifted(jnp.stack(pieces), "c", 1)
    out = pl.pallas_call(
        place_kernel,
        out_shape=jax.ShapeDtypeStruct((tokens, width), BF16),
        in_specs=[pl.BlockSpec(memory_space=pltpu.SMEM)] + vmem(5),
        out_specs=pl.BlockSpec(memory_space=pltpu.VMEM),
        name="place",
    )(at, *pieces, ig_other)

    groups = lax.axis_size(REP_FS)
    last = part // 8
    tail = pl.BlockSpec((8, width), lambda i: (last, 0))
    gain_chip = pl.pallas_call(
        gain_kernel,
        out_shape=jax.ShapeDtypeStruct((groups, 1, width), F32),
        grid=(1,),
        in_specs=[tail] * 4 + [pl.BlockSpec((4, 8, width), lambda i: (0, last, 0))],
        out_specs=pl.BlockSpec((groups, 1, width), lambda i: (0, 0, 0)),
        name="gain",
    )(*pieces, ig_other)
    gain_all = exchanged(gain_chip, REP_FS)
    gain_gradient = jnp.sum(gain_all, axis=(0, 1))

    dy = jnp.sum(dy.astype(F32), axis=0).astype(BF16)
    dz = rolled(dy, (nz - zl) % nz).reshape(nz, 2, rows // 2, units).transpose(1, 0, 2, 3)
    dz = dz.reshape(2 * nz, rows // 2, units)
    dz = exchanged(dz, RING)
    own = jnp.sum(dz.astype(F32), axis=0)
    far = shifted(own, "rep", 1)
    pair = rolled(jnp.stack([own, far]), rep)
    d_down = pair.reshape(rows, units)
    return (out, gain_gradient, d_down)


def solution(mesh):
    torus = Mesh(
        mesh.devices.reshape(mesh.shape["rep"], 8, 4, 4, 2),
        ("rep", "fs_0", "fs_1", "x", "c"),
    )
    return jax.shard_map(
        work,
        mesh=torus,
        in_specs=(P(REP_FS, None), P(), P(FS, TP), P(FS, TP), P(FS, TP), P(REP_FS, None)),
        out_specs=(P(REP_FS, None), P(), P(FS, TP)),
        check_vma=False,
    )
```

```python
import jax
import jax.numpy as jnp
from jax import lax
from jax.experimental import pallas as pl
from jax.experimental.pallas import tpu as pltpu
from jax.sharding import Mesh
from jax.sharding import PartitionSpec as P

FS = ("fs_0", "fs_1")
REP_FS = ("rep", "fs_0", "fs_1")
TP = ("x", "c")
RING = ("rep", "fs_0")
EPS = 1e-06
F32 = jnp.float32
BF16 = jnp.bfloat16


def shifted(v, axis, by):
    n = lax.axis_size(axis)
    return lax.ppermute(v, axis, [(i, (i + by) % n) for i in range(n)])


def exchanged(v, axis):
    return lax.all_to_all(v, axis, 0, 0, tiled=True)


def from_all(v, axis):
    n = lax.axis_size(axis)
    return exchanged(jnp.broadcast_to(v[None], (n, *v.shape)), axis)


def rolled(v, start):
    return lax.dynamic_slice_in_dim(jnp.concatenate([v, v], axis=0), start, v.shape[0], axis=0)


def blocks_of(refs):
    for d in range(4):
        yield d, 0, refs[d]
    yield 4, 0, refs[4]
    yield 4, refs[4].shape[0], refs[5]
    for d in range(5, 8):
        yield d, 0, refs[d + 1]


def prepare_tokens(at_ref, x_ref, gain_ref, out_ref):
    nz, _, cols = out_ref.shape
    v = x_ref[...].astype(F32)
    inv = lax.rsqrt(jnp.mean(v * v, axis=-1, keepdims=True) + EPS)
    for d in range(nz):
        own = pl.ds(pl.multiple_of(((at_ref[0] + d) % nz) * cols, cols), cols)
        part = x_ref[:, own].astype(F32)
        out_ref[d] = (part * inv * gain_ref[:, own]).astype(BF16)


def prepare_cotangent(at_ref, lo_ref, hi_ref, out_ref, turned_ref):
    nz, _, cols = out_ref.shape
    for d in range(nz):
        own = pl.ds(pl.multiple_of(((at_ref[0] + d) % nz) * cols, cols), cols)
        part = jnp.concatenate([lo_ref[:, own], hi_ref[:, own]], axis=0)
        out_ref[d] = part
        turned_ref[d] = part.T


def grad_kernel(x_ref, c_ref, gain_ref, *refs):
    w_refs, (mine_ref, other_ref, hid_ref, sum_ref) = refs[:9], refs[9:]
    units = hid_ref.shape[1]
    nx, _, part, _ = mine_ref.shape
    gu = dh = None
    for d, lo, w in blocks_of(w_refs):
        rows = w.shape[0]
        a = jnp.dot(x_ref[d, :, lo : lo + rows], w[:, : 2 * units], preferred_element_type=F32)
        b = jnp.dot(c_ref[d, :, lo : lo + rows], w[:, 2 * units :], preferred_element_type=F32)
        gu = a if gu is None else gu + a
        dh = b if dh is None else dh + b
    gate, up = gu[:, :units], gu[:, units:]
    dh = 0.5 * dh
    sig = jax.nn.sigmoid(gate)
    act = gate * sig
    hid_ref[...] = (act * up).astype(BF16)
    d_gate = (dh * up * sig * (1.0 + gate * (1.0 - sig))).astype(BF16)
    d_up = (dh * act).astype(BF16)
    both = jnp.concatenate([d_gate, d_up], axis=1)
    for d, lo, w in blocks_of(w_refs):
        rows = w.shape[0]
        out = lax.dot_general(
            both, w[:, : 2 * units], (((1,), (1,)), ((), ())), preferred_element_type=F32
        )
        terms = x_ref[d, :, lo : lo + rows].astype(F32) * out
        sums = jnp.sum(terms, axis=0, keepdims=True)
        sum_ref[d, :, lo : lo + rows] = sums / gain_ref[d, :, lo : lo + rows]
        out = out.astype(BF16)
        for k in range(nx):
            mine_ref[k, d, :, lo : lo + rows] = out[k * part : (k + 1) * part]
            other_ref[k, d, :, lo : lo + rows] = out[(nx + k) * part : (nx + k + 1) * part]


def down_kernel(ct_ref, hid_ref, sum_ref, out_ref):
    ny, nz, longer, units = out_ref.shape
    rows = longer - 8
    cols = sum_ref.shape[2]
    for d in range(nz):
        res = jnp.dot(ct_ref[d], hid_ref[...], preferred_element_type=F32)
        res = (0.5 * res).astype(BF16)
        sums = sum_ref[d]
        high = sums.astype(BF16)
        left = sums - high.astype(F32)
        mid = left.astype(BF16)
        low = (left - mid.astype(F32)).astype(BF16)
        extra = jnp.concatenate([high, mid, low, jnp.zeros((5, cols), BF16)], axis=0)
        extra = jnp.concatenate([extra, jnp.zeros((8, units - cols), BF16)], axis=1)
        for y in range(ny):
            out_ref[y, d, :rows] = res[y * rows : (y + 1) * rows]
            out_ref[y, d, rows:] = extra


def rows_kernel(at_ref, got_ref, out_ref):
    ny, nz, longer, _ = got_ref.shape
    rows = longer - 8
    half = rows // 2
    sums = []
    for d in range(nz):
        total = got_ref[0, d].astype(F32)
        for k in range(1, ny):
            total = total + got_ref[k, d].astype(F32)
        part = total[:rows].astype(BF16)
        to = (at_ref[0] + d) % nz
        out_ref[to, :half] = part[:half]
        out_ref[nz + to, :half] = part[half:]
        sums.append(jnp.sum(total[rows:], axis=0, keepdims=True))
    extra = jnp.concatenate(sums, axis=0)
    extra = pltpu.roll(extra, at_ref[0], 0).astype(BF16)
    for k in range(2 * nz):
        out_ref[k, half:] = extra


def ring_kernel(got_ref, out_ref, sum_ref):
    half = out_ref.shape[0]
    cols = sum_ref.shape[2]
    total = got_ref[0].astype(F32)
    for k in range(1, got_ref.shape[0]):
        total = total + got_ref[k].astype(F32)
    out_ref[...] = total[:half]
    for k in range(sum_ref.shape[0]):
        sum_ref[k] = total[half:, :cols]


def chip_kernel(mine_ref, theirs_ref, *out_refs):
    for k, out_ref in enumerate(out_refs):
        out_ref[...] = (mine_ref[k].astype(F32) + theirs_ref[k].astype(F32)).astype(BF16)


def finish_kernel(at_ref, got0, got1, got2, got3, x_ref, c_ref, gain_ref, out_ref, dn_ref):
    nz, _, cols = got0.shape
    for d in range(nz):
        own = pl.ds(pl.multiple_of(((at_ref[0] + d) % nz) * cols, cols), cols)
        total = got0[d].astype(F32)
        for got in (got1, got2, got3):
            total = total + got[d].astype(F32)
        dn_ref[:, own] = total.astype(BF16)
    v = x_ref[...].astype(F32)
    inv = lax.rsqrt(jnp.mean(v * v, axis=-1, keepdims=True) + EPS)
    xhat = v * inv
    dn = dn_ref[...].astype(F32)
    gs = gain_ref[...] * dn
    m = jnp.mean(gs * xhat, axis=-1, keepdims=True)
    out_ref[...] = (c_ref[...].astype(F32) + inv * (gs - xhat * m)).astype(BF16)


def place_kernel(at_ref, p0, p1, p2, p3, other_ref, out_ref):
    n = 4
    part = out_ref.shape[0] // (2 * n)
    for k, piece in enumerate((p0, p1, p2, p3)):
        spot = (at_ref[2] + k) % n
        own = pl.multiple_of((at_ref[1] * n + spot) * part, part)
        far = pl.multiple_of(((1 - at_ref[1]) * n + spot) * part, part)
        out_ref[pl.ds(own, part), :] = piece[:part]
        out_ref[pl.ds(far, part), :] = other_ref[k, :part]


def near(*arrays):
    return [pltpu.with_memory_space_constraint(a, pltpu.VMEM) for a in arrays]


def vmem(n):
    return [pl.BlockSpec(memory_space=pltpu.VMEM)] * n


def work(inputs, gain, gate_weight, up_weight, down_weight, cotangent):
    nz, ny, nx = lax.axis_size("fs_0"), lax.axis_size("fs_1"), lax.axis_size("x")
    rep, zl = lax.axis_index("rep"), lax.axis_index("fs_0")
    x, c = lax.axis_index("x"), lax.axis_index("c")
    tokens, width = inputs.shape
    rows, units = gate_weight.shape
    cols = width // nz
    part = tokens // 2 // nx
    gain2 = gain[None]
    at = jnp.stack([zl, c, x]).astype(jnp.int32)

    w = jnp.concatenate([gate_weight, up_weight, down_weight], axis=1)
    w0 = from_all(w, "fs_1").reshape(ny * rows, 3 * units)
    fwd, bwd = [w0], [w0]
    for _ in range(3):
        fwd.append(shifted(fwd[-1], RING, 1))
        bwd.append(shifted(bwd[-1], RING, -1))
    mid = cols // 2
    last_f = shifted(fwd[-1][:mid], RING, 1)
    last_b = shifted(bwd[-1][mid:], RING, -1)
    weights = [w0, bwd[1], bwd[2], bwd[3], last_f, last_b, fwd[3], fwd[2], fwd[1]]

    def spot(i, at):
        return ((i // nx + at[1]) % 2) * nx + (i + at[2]) % nx

    xr = pl.pallas_call(
        prepare_tokens,
        out_shape=jax.ShapeDtypeStruct((nz, tokens, cols), BF16),
        grid_spec=pltpu.PrefetchScalarGridSpec(
            num_scalar_prefetch=1,
            grid=(2 * nx,),
            in_specs=[
                pl.BlockSpec((part, width), lambda i, at: (spot(i, at), 0)),
                pl.BlockSpec((1, width), lambda i, at: (0, 0)),
            ],
            out_specs=pl.BlockSpec((nz, part, cols), lambda i, at: (0, i, 0)),
        ),
        name="prepare_x",
    )(at, inputs, gain2)
    cr, ct = pl.pallas_call(
        prepare_cotangent,
        out_shape=(
            jax.ShapeDtypeStruct((nz, tokens, cols), BF16),
            jax.ShapeDtypeStruct((nz, cols, tokens), BF16),
        ),
        grid_spec=pltpu.PrefetchScalarGridSpec(
            num_scalar_prefetch=1,
            grid=(nx,),
            in_specs=[
                pl.BlockSpec((part, width), lambda i, at: (spot(2 * i, at), 0)),
                pl.BlockSpec((part, width), lambda i, at: (spot(2 * i + 1, at), 0)),
            ],
            out_specs=(
                pl.BlockSpec((nz, 2 * part, cols), lambda i, at: (0, i, 0)),
                pl.BlockSpec((nz, cols, 2 * part), lambda i, at: (0, 0, i)),
            ),
        ),
        name="prepare_c",
    )(at, cotangent, cotangent)

    gain_ring = rolled(gain.reshape(nz, 1, cols), zl)
    mine, other, hidden, sums = pl.pallas_call(
        grad_kernel,
        out_shape=(
            jax.ShapeDtypeStruct((nx, nz, part, cols), BF16),
            jax.ShapeDtypeStruct((nx, nz, part, cols), BF16),
            jax.ShapeDtypeStruct((tokens, units), BF16),
            jax.ShapeDtypeStruct((nz, 1, cols), F32),
        ),
        in_specs=vmem(12),
        out_specs=tuple(vmem(4)),
        name="grad",
    )(xr, cr, gain_ring, *weights[:4], *near(last_f, last_b), *weights[6:])
    theirs = shifted(other, "c", 1)
    (dd,) = pl.pallas_call(
        down_kernel,
        out_shape=(jax.ShapeDtypeStruct((ny, nz, rows + 8, units), BF16),),
        in_specs=vmem(3),
        out_specs=tuple(vmem(1)),
        name="down",
    )(ct, hidden, sums)
    dy = exchanged(dd, "fs_1")

    chunk = jax.ShapeDtypeStruct((nz, part, cols), BF16)
    chip = pl.pallas_call(
        chip_kernel,
        out_shape=(chunk,) * 4,
        in_specs=vmem(2),
        out_specs=tuple(vmem(4)),
        name="chip",
    )(mine, *near(theirs))
    got = [chip[0]]
    for k in (1, 2, 3):
        got.append(shifted(chip[k], "x", k))
    own = pl.BlockSpec((part, width), lambda i, at: (at[1] * nx + at[2], 0))
    ig = pl.pallas_call(
        finish_kernel,
        out_shape=jax.ShapeDtypeStruct((part, width), BF16),
        grid_spec=pltpu.PrefetchScalarGridSpec(
            num_scalar_prefetch=1,
            grid=(1,),
            in_specs=vmem(4) + [own, own, pl.BlockSpec((1, width), lambda i, at: (0, 0))],
            out_specs=pl.BlockSpec((part, width), lambda i, at: (0, 0)),
            scratch_shapes=[pltpu.VMEM((part, width), BF16)],
        ),
        name="finish",
    )(at, got[0], *near(*got[1:]), inputs, cotangent, gain2)
    pieces = [ig]
    for k in (1, 2, 3):
        pieces.append(shifted(ig, "x", -k))
    ig_other = shifted(jnp.stack(pieces), "c", 1)
    out = pl.pallas_call(
        place_kernel,
        out_shape=jax.ShapeDtypeStruct((tokens, width), BF16),
        in_specs=[pl.BlockSpec(memory_space=pltpu.SMEM)] + vmem(5),
        out_specs=pl.BlockSpec(memory_space=pltpu.VMEM),
        name="place",
    )(at, pieces[0], *near(*pieces[1:], ig_other))

    dz = pl.pallas_call(
        rows_kernel,
        out_shape=jax.ShapeDtypeStruct((2 * nz, rows // 2 + 8, units), BF16),
        in_specs=[pl.BlockSpec(memory_space=pltpu.SMEM)] + vmem(1),
        out_specs=pl.BlockSpec(memory_space=pltpu.VMEM),
        name="ysum",
    )(at, *near(dy))
    dz = exchanged(dz, RING)
    own, gain_own = pl.pallas_call(
        ring_kernel,
        out_shape=(
            jax.ShapeDtypeStruct((rows // 2, units), F32),
            jax.ShapeDtypeStruct((lax.axis_size(TP), nz, cols), F32),
        ),
        in_specs=vmem(1),
        out_specs=tuple(vmem(2)),
        name="zsum",
    )(*near(dz))
    gain_all = exchanged(gain_own, TP)
    gain_gradient = jnp.sum(gain_all, axis=0).reshape(width)
    far = shifted(own, "rep", 1)
    pair = rolled(jnp.stack([own, far]), rep)
    d_down = pair.reshape(rows, units)
    return (out, gain_gradient, d_down)


def solution(mesh):
    torus = Mesh(
        mesh.devices.reshape(mesh.shape["rep"], 8, 4, 4, 2),
        ("rep", "fs_0", "fs_1", "x", "c"),
    )
    return jax.shard_map(
        work,
        mesh=torus,
        in_specs=(P(REP_FS, None), P(), P(FS, TP), P(FS, TP), P(FS, TP), P(REP_FS, None)),
        out_specs=(P(REP_FS, None), P(), P(FS, TP)),
        check_vma=False,
    )
```

```python
import jax
import jax.numpy as jnp
from jax import lax
from jax.experimental import pallas as pl
from jax.experimental.pallas import tpu as pltpu
from jax.sharding import Mesh
from jax.sharding import PartitionSpec as P

FS = ("fs_0", "fs_1")
REP_FS = ("rep", "fs_0", "fs_1")
TP = ("x", "c")
RING = ("rep", "fs_0")
EPS = 1e-06
EARLY = (0, 1, 7, 2, 6)
F32 = jnp.float32
BF16 = jnp.bfloat16


def shifted(v, axis, by):
    n = lax.axis_size(axis)
    return lax.ppermute(v, axis, [(i, (i + by) % n) for i in range(n)])


def exchanged(v, axis):
    return lax.all_to_all(v, axis, 0, 0, tiled=True)


def from_all(v, axis):
    n = lax.axis_size(axis)
    return exchanged(jnp.broadcast_to(v[None], (n, *v.shape)), axis)


def rolled(v, start):
    return lax.dynamic_slice_in_dim(jnp.concatenate([v, v], axis=0), start, v.shape[0], axis=0)


def prepare_tokens(at_ref, x_ref, gain_ref, out_ref):
    nz, _, cols = out_ref.shape
    v = x_ref[...].astype(F32)
    inv = lax.rsqrt(jnp.mean(v * v, axis=-1, keepdims=True) + EPS)
    for d in range(nz):
        own = pl.ds(pl.multiple_of(((at_ref[0] + d) % nz) * cols, cols), cols)
        part = x_ref[:, own].astype(F32)
        out_ref[d] = (part * inv * gain_ref[:, own]).astype(BF16)


def prepare_cotangent(at_ref, lo_ref, hi_ref, out_ref, turned_ref):
    nz, _, cols = out_ref.shape
    for d in range(nz):
        own = pl.ds(pl.multiple_of(((at_ref[0] + d) % nz) * cols, cols), cols)
        part = jnp.concatenate([lo_ref[:, own], hi_ref[:, own]], axis=0)
        out_ref[d] = part
        turned_ref[d] = part.T


def forward_kernel(x_ref, c_ref, *refs):
    w_refs, acc_ref = refs[:-1], refs[-1]
    units = acc_ref.shape[1] // 3
    gu = dh = None
    for d, w in zip(EARLY, w_refs):
        a = jnp.dot(x_ref[d], w[:, : 2 * units], preferred_element_type=F32)
        b = jnp.dot(c_ref[d], w[:, 2 * units :], preferred_element_type=F32)
        gu = a if gu is None else gu + a
        dh = b if dh is None else dh + b
    acc_ref[:, : 2 * units] = gu
    acc_ref[:, 2 * units :] = dh


def grad_kernel(gain_ref, lo_ref, hi_ref, acc_hbm, x_hbm, c_hbm, ct_hbm, *refs):
    w_hbm, (mine_hbm, other_hbm, dd_hbm) = refs[:7], refs[7:10]
    acc, xv, cv, ctv, wv, ov, dv, sems = refs[10:]
    units = acc.shape[1] // 3
    nz, _, cols = xv.shape
    ny, _, longer, _ = dv.shape
    nx, part = mine_hbm.shape[0], mine_hbm.shape[2]
    rows = longer - 8
    used = [0]

    def begin(src, dst):
        copy = pltpu.make_async_copy(src, dst, sems.at[used[0]])
        used[0] += 1
        copy.start()
        return copy

    slot = {0: 0, 1: 1, 2: 2, 3: 3, 5: 4, 6: 5, 7: 6}
    acc_in = begin(acc_hbm, acc)
    x_in, c_in, w_in = {}, {}, {}
    for d in (3, 5):
        w_in[d] = begin(w_hbm[slot[d]], wv.at[slot[d]])
        x_in[d] = begin(x_hbm.at[d], xv.at[d])
        c_in[d] = begin(c_hbm.at[d], cv.at[d - 3])
    x_in[4] = begin(x_hbm.at[4], xv.at[4])
    c_in[4] = begin(c_hbm.at[4], cv.at[1])
    for d in EARLY:
        w_in[d] = begin(w_hbm[slot[d]], wv.at[slot[d]])
        x_in[d] = begin(x_hbm.at[d], xv.at[d])
    ct_in = begin(ct_hbm, ctv)

    half = cols // 2
    halves = ((lo_ref, slice(0, half)), (hi_ref, slice(half, cols)))
    acc_in.wait()
    gu, dh = acc[:, : 2 * units], acc[:, 2 * units :]
    for d in (3, 5):
        w_in[d].wait()
        x_in[d].wait()
        c_in[d].wait()
        w = wv.at[slot[d]]
        gu = gu + jnp.dot(xv[d], w[:, : 2 * units], preferred_element_type=F32)
        dh = dh + jnp.dot(cv[d - 3], w[:, 2 * units :], preferred_element_type=F32)
    x_in[4].wait()
    c_in[4].wait()
    for w, at in halves:
        gu = gu + jnp.dot(xv[4, :, at], w[:, : 2 * units], preferred_element_type=F32)
        dh = dh + jnp.dot(cv[1, :, at], w[:, 2 * units :], preferred_element_type=F32)
    gate, up = gu[:, :units], gu[:, units:]
    dh = 0.5 * dh
    sig = jax.nn.sigmoid(gate)
    act = gate * sig
    hidden = (act * up).astype(BF16)
    d_gate = (dh * up * sig * (1.0 + gate * (1.0 - sig))).astype(BF16)
    d_up = (dh * act).astype(BF16)
    both = jnp.concatenate([d_gate, d_up], axis=1)
    out_copies = []
    sums = {}
    for d in (4, 3, 5) + EARLY:
        if d in EARLY:
            w_in[d].wait()
            x_in[d].wait()
        pieces = halves if d == 4 else ((wv.at[slot[d]], slice(0, cols)),)
        got = []
        for w, at in pieces:
            out = lax.dot_general(
                both, w[:, : 2 * units], (((1,), (1,)), ((), ())), preferred_element_type=F32
            )
            terms = jnp.sum(xv[d, :, at].astype(F32) * out, axis=0, keepdims=True)
            got.append(terms / gain_ref[d, :, at])
            out = out.astype(BF16)
            for k in range(2 * nx):
                ov[k, d, :, at] = out[k * part : (k + 1) * part]
        sums[d] = got[0] if len(got) == 1 else jnp.concatenate(got, axis=1)
        out_copies.append(begin(ov.at[pl.ds(nx, nx), d], other_hbm.at[:, d]))
        out_copies.append(begin(ov.at[pl.ds(0, nx), d], mine_hbm.at[:, d]))
    ct_in.wait()
    for d in range(nz):
        res = jnp.dot(ctv[d], hidden, preferred_element_type=F32)
        res = (0.5 * res).astype(BF16)
        high = sums[d].astype(BF16)
        left = sums[d] - high.astype(F32)
        mid = left.astype(BF16)
        low = (left - mid.astype(F32)).astype(BF16)
        extra = jnp.concatenate([high, mid, low, jnp.zeros((5, cols), BF16)], axis=0)
        extra = jnp.concatenate([extra, jnp.zeros((8, units - cols), BF16)], axis=1)
        for y in range(ny):
            dv[y, d, :rows] = res[y * rows : (y + 1) * rows]
            dv[y, d, rows:] = extra
        out_copies.append(begin(dv.at[:, d], dd_hbm.at[:, d]))
    for copy in out_copies:
        copy.wait()


def rows_kernel(at_ref, got_ref, out_ref):
    ny, nz, longer, _ = got_ref.shape
    rows = longer - 8
    half = rows // 2
    sums = []
    for d in range(nz):
        total = got_ref[0, d].astype(F32)
        for k in range(1, ny):
            total = total + got_ref[k, d].astype(F32)
        part = total[:rows].astype(BF16)
        to = (at_ref[0] + d) % nz
        out_ref[to, :half] = part[:half]
        out_ref[nz + to, :half] = part[half:]
        sums.append(jnp.sum(total[rows:], axis=0, keepdims=True))
    extra = jnp.concatenate(sums, axis=0)
    extra = pltpu.roll(extra, at_ref[0], 0).astype(BF16)
    for k in range(2 * nz):
        out_ref[k, half:] = extra


def ring_kernel(got_ref, out_ref, sum_ref):
    half = out_ref.shape[0]
    cols = sum_ref.shape[2]
    total = got_ref[0].astype(F32)
    for k in range(1, got_ref.shape[0]):
        total = total + got_ref[k].astype(F32)
    out_ref[...] = total[:half]
    for k in range(sum_ref.shape[0]):
        sum_ref[k] = total[half:, :cols]


def chip_kernel(mine_ref, theirs_ref, *out_refs):
    for k, out_ref in enumerate(out_refs):
        out_ref[...] = (mine_ref[k].astype(F32) + theirs_ref[k].astype(F32)).astype(BF16)


def finish_kernel(at_ref, got0, got1, got2, got3, x_ref, c_ref, gain_ref, out_ref, dn_ref):
    nz, _, cols = got0.shape
    for d in range(nz):
        own = pl.ds(pl.multiple_of(((at_ref[0] + d) % nz) * cols, cols), cols)
        total = got0[d].astype(F32)
        for got in (got1, got2, got3):
            total = total + got[d].astype(F32)
        dn_ref[:, own] = total.astype(BF16)
    v = x_ref[...].astype(F32)
    inv = lax.rsqrt(jnp.mean(v * v, axis=-1, keepdims=True) + EPS)
    xhat = v * inv
    dn = dn_ref[...].astype(F32)
    gs = gain_ref[...] * dn
    m = jnp.mean(gs * xhat, axis=-1, keepdims=True)
    out_ref[...] = (c_ref[...].astype(F32) + inv * (gs - xhat * m)).astype(BF16)


def place_kernel(at_ref, p0, p1, p2, p3, other_ref, out_ref):
    n = 4
    part = out_ref.shape[0] // (2 * n)
    for k, piece in enumerate((p0, p1, p2, p3)):
        spot = (at_ref[2] + k) % n
        own = pl.multiple_of((at_ref[1] * n + spot) * part, part)
        far = pl.multiple_of(((1 - at_ref[1]) * n + spot) * part, part)
        out_ref[pl.ds(own, part), :] = piece[:part]
        out_ref[pl.ds(far, part), :] = other_ref[k, :part]


def near(*arrays):
    return [pltpu.with_memory_space_constraint(a, pltpu.VMEM) for a in arrays]


def vmem(n):
    return [pl.BlockSpec(memory_space=pltpu.VMEM)] * n


def work(inputs, gain, gate_weight, up_weight, down_weight, cotangent):
    nz, ny, nx = lax.axis_size("fs_0"), lax.axis_size("fs_1"), lax.axis_size("x")
    rep, zl = lax.axis_index("rep"), lax.axis_index("fs_0")
    x, c = lax.axis_index("x"), lax.axis_index("c")
    tokens, width = inputs.shape
    rows, units = gate_weight.shape
    cols = width // nz
    part = tokens // 2 // nx
    gain2 = gain[None]
    at = jnp.stack([zl, c, x]).astype(jnp.int32)

    w = jnp.concatenate([gate_weight, up_weight, down_weight], axis=1)
    w0 = from_all(w, "fs_1").reshape(ny * rows, 3 * units)
    fwd, bwd = [w0], [w0]
    for _ in range(3):
        fwd.append(shifted(fwd[-1], RING, 1))
        bwd.append(shifted(bwd[-1], RING, -1))
    mid = cols // 2
    last_f = shifted(fwd[-1][:mid], RING, 1)
    last_b = shifted(bwd[-1][mid:], RING, -1)
    weights = [w0, bwd[1], bwd[2], bwd[3], fwd[3], fwd[2], fwd[1]]

    def spot(i, at):
        return ((i // nx + at[1]) % 2) * nx + (i + at[2]) % nx

    xr = pl.pallas_call(
        prepare_tokens,
        out_shape=jax.ShapeDtypeStruct((nz, tokens, cols), BF16),
        grid_spec=pltpu.PrefetchScalarGridSpec(
            num_scalar_prefetch=1,
            grid=(2 * nx,),
            in_specs=[
                pl.BlockSpec((part, width), lambda i, at: (spot(i, at), 0)),
                pl.BlockSpec((1, width), lambda i, at: (0, 0)),
            ],
            out_specs=pl.BlockSpec((nz, part, cols), lambda i, at: (0, i, 0)),
        ),
        name="prepare_x",
    )(at, inputs, gain2)
    cr, ct = pl.pallas_call(
        prepare_cotangent,
        out_shape=(
            jax.ShapeDtypeStruct((nz, tokens, cols), BF16),
            jax.ShapeDtypeStruct((nz, cols, tokens), BF16),
        ),
        grid_spec=pltpu.PrefetchScalarGridSpec(
            num_scalar_prefetch=1,
            grid=(nx,),
            in_specs=[
                pl.BlockSpec((part, width), lambda i, at: (spot(2 * i, at), 0)),
                pl.BlockSpec((part, width), lambda i, at: (spot(2 * i + 1, at), 0)),
            ],
            out_specs=(
                pl.BlockSpec((nz, 2 * part, cols), lambda i, at: (0, i, 0)),
                pl.BlockSpec((nz, cols, 2 * part), lambda i, at: (0, 0, i)),
            ),
        ),
        name="prepare_c",
    )(at, cotangent, cotangent)

    gain_ring = rolled(gain.reshape(nz, 1, cols), zl)
    acc = pl.pallas_call(
        forward_kernel,
        out_shape=jax.ShapeDtypeStruct((tokens, 3 * units), F32),
        in_specs=vmem(7),
        out_specs=pl.BlockSpec(memory_space=pltpu.VMEM),
        name="forward",
    )(xr, cr, w0, bwd[1], fwd[1], bwd[2], fwd[2])
    anywhere = pl.BlockSpec(memory_space=pl.ANY)
    mine, other, dd = pl.pallas_call(
        grad_kernel,
        out_shape=(
            jax.ShapeDtypeStruct((nx, nz, part, cols), BF16),
            jax.ShapeDtypeStruct((nx, nz, part, cols), BF16),
            jax.ShapeDtypeStruct((ny, nz, rows + 8, units), BF16),
        ),
        in_specs=vmem(3) + [anywhere] * 11,
        out_specs=(anywhere,) * 3,
        scratch_shapes=[
            pltpu.VMEM((tokens, 3 * units), F32),
            pltpu.VMEM((nz, tokens, cols), BF16),
            pltpu.VMEM((3, tokens, cols), BF16),
            pltpu.VMEM((nz, cols, tokens), BF16),
            pltpu.VMEM((7, cols, 3 * units), BF16),
            pltpu.VMEM((2 * nx, nz, part, cols), BF16),
            pltpu.VMEM((ny, nz, rows + 8, units), BF16),
            pltpu.SemaphoreType.DMA((48,)),
        ],
        name="grad",
    )(gain_ring, *near(last_f, last_b), acc, xr, cr, ct, *weights)
    theirs = shifted(other, "c", 1)
    dy = exchanged(dd, "fs_1")

    chunk = jax.ShapeDtypeStruct((nz, part, cols), BF16)
    chip = pl.pallas_call(
        chip_kernel,
        out_shape=(chunk,) * 4,
        in_specs=vmem(2),
        out_specs=tuple(vmem(4)),
        name="chip",
    )(mine, *near(theirs))
    got = [chip[0]]
    for k in (1, 2, 3):
        got.append(shifted(chip[k], "x", k))
    own = pl.BlockSpec((part, width), lambda i, at: (at[1] * nx + at[2], 0))
    ig = pl.pallas_call(
        finish_kernel,
        out_shape=jax.ShapeDtypeStruct((part, width), BF16),
        grid_spec=pltpu.PrefetchScalarGridSpec(
            num_scalar_prefetch=1,
            grid=(1,),
            in_specs=vmem(4) + [own, own, pl.BlockSpec((1, width), lambda i, at: (0, 0))],
            out_specs=pl.BlockSpec((part, width), lambda i, at: (0, 0)),
            scratch_shapes=[pltpu.VMEM((part, width), BF16)],
        ),
        name="finish",
    )(at, got[0], *near(*got[1:]), inputs, cotangent, gain2)
    pieces = [ig]
    for k in (1, 2, 3):
        pieces.append(shifted(ig, "x", -k))
    ig_other = shifted(jnp.stack(pieces), "c", 1)
    out = pl.pallas_call(
        place_kernel,
        out_shape=jax.ShapeDtypeStruct((tokens, width), BF16),
        in_specs=[pl.BlockSpec(memory_space=pltpu.SMEM)] + vmem(5),
        out_specs=pl.BlockSpec(memory_space=pltpu.VMEM),
        name="place",
    )(at, pieces[0], *near(*pieces[1:], ig_other))

    dz = pl.pallas_call(
        rows_kernel,
        out_shape=jax.ShapeDtypeStruct((2 * nz, rows // 2 + 8, units), BF16),
        in_specs=[pl.BlockSpec(memory_space=pltpu.SMEM)] + vmem(1),
        out_specs=pl.BlockSpec(memory_space=pltpu.VMEM),
        name="ysum",
    )(at, *near(dy))
    dz = exchanged(dz, RING)
    own, gain_own = pl.pallas_call(
        ring_kernel,
        out_shape=(
            jax.ShapeDtypeStruct((rows // 2, units), F32),
            jax.ShapeDtypeStruct((lax.axis_size(TP), nz, cols), F32),
        ),
        in_specs=vmem(1),
        out_specs=tuple(vmem(2)),
        name="zsum",
    )(*near(dz))
    gain_all = exchanged(gain_own, TP)
    gain_gradient = jnp.sum(gain_all, axis=0).reshape(width)
    far = shifted(own, "rep", 1)
    pair = rolled(jnp.stack([own, far]), rep)
    d_down = pair.reshape(rows, units)
    return (out, gain_gradient, d_down)


def solution(mesh):
    torus = Mesh(
        mesh.devices.reshape(mesh.shape["rep"], 8, 4, 4, 2),
        ("rep", "fs_0", "fs_1", "x", "c"),
    )
    return jax.shard_map(
        work,
        mesh=torus,
        in_specs=(P(REP_FS, None), P(), P(FS, TP), P(FS, TP), P(FS, TP), P(REP_FS, None)),
        out_specs=(P(REP_FS, None), P(), P(FS, TP)),
        check_vma=False,
    )
```

```python
import jax
import jax.numpy as jnp
from jax import lax
from jax.experimental import pallas as pl
from jax.experimental.pallas import tpu as pltpu
from jax.sharding import Mesh
from jax.sharding import PartitionSpec as P

FS = ("fs_0", "fs_1")
REP_FS = ("rep", "fs_0", "fs_1")
TP = ("x", "c")
RING = ("rep", "fs_0")
EPS = 1e-06
EARLY = (0, 1, 7, 2, 6)
F32 = jnp.float32
BF16 = jnp.bfloat16


def shifted(v, axis, by):
    n = lax.axis_size(axis)
    return lax.ppermute(v, axis, [(i, (i + by) % n) for i in range(n)])


def exchanged(v, axis):
    return lax.all_to_all(v, axis, 0, 0, tiled=True)


def from_all(v, axis):
    n = lax.axis_size(axis)
    return exchanged(jnp.broadcast_to(v[None], (n, *v.shape)), axis)


def rolled(v, start):
    return lax.dynamic_slice_in_dim(jnp.concatenate([v, v], axis=0), start, v.shape[0], axis=0)


def prepare_tokens(at_ref, x_ref, gain_ref, out_ref):
    nz, _, cols = out_ref.shape
    v = x_ref[...].astype(F32)
    inv = lax.rsqrt(jnp.mean(v * v, axis=-1, keepdims=True) + EPS)
    for d in range(nz):
        own = pl.ds(pl.multiple_of(((at_ref[0] + d) % nz) * cols, cols), cols)
        part = x_ref[:, own].astype(F32)
        out_ref[d] = (part * inv * gain_ref[:, own]).astype(BF16)


def prepare_cotangent(at_ref, lo_ref, hi_ref, out_ref, turned_ref):
    nz, _, cols = out_ref.shape
    for d in range(nz):
        own = pl.ds(pl.multiple_of(((at_ref[0] + d) % nz) * cols, cols), cols)
        part = jnp.concatenate([lo_ref[:, own], hi_ref[:, own]], axis=0)
        out_ref[d] = part
        turned_ref[d] = part.T


def forward_kernel(x_ref, c_ref, *refs):
    acc_ref = refs[-1]
    units = acc_ref.shape[1] // 3
    gu = dh = None
    for i, d in enumerate(EARLY):
        a = jnp.dot(x_ref[d], refs[i][...], preferred_element_type=F32)
        b = jnp.dot(c_ref[d], refs[len(EARLY) + i][...], preferred_element_type=F32)
        gu = a if gu is None else gu + a
        dh = b if dh is None else dh + b
    acc_ref[:, : 2 * units] = gu
    acc_ref[:, 2 * units :] = dh


def grad_kernel(gain_ref, gu4_ref, down4_ref, acc_hbm, x_hbm, c_hbm, ct_hbm, *refs):
    w_hbm, down_hbm, (mine_hbm, other_hbm, dd_hbm) = refs[:7], refs[7:9], refs[9:12]
    acc, xv, cv, ctv, wv, dwv, ov, dv, sems = refs[12:]
    units = acc.shape[1] // 3
    nz, _, cols = xv.shape
    ny, _, longer, _ = dv.shape
    nx, part = mine_hbm.shape[0], mine_hbm.shape[2]
    rows = longer - 8
    used = [0]

    def begin(src, dst):
        copy = pltpu.make_async_copy(src, dst, sems.at[used[0]])
        used[0] += 1
        copy.start()
        return copy

    slot = {0: 0, 1: 1, 2: 2, 3: 3, 5: 4, 6: 5, 7: 6}
    acc_in = begin(acc_hbm, acc)
    x_in, c_in, w_in, down_in = {}, {}, {}, {}
    for d in (3, 5):
        w_in[d] = begin(w_hbm[slot[d]], wv.at[slot[d]])
        x_in[d] = begin(x_hbm.at[d], xv.at[d])
        c_in[d] = begin(c_hbm.at[d], cv.at[d - 3])
        down_in[d] = begin(down_hbm[(d - 3) // 2], dwv.at[(d - 3) // 2])
    x_in[4] = begin(x_hbm.at[4], xv.at[4])
    c_in[4] = begin(c_hbm.at[4], cv.at[1])
    for d in EARLY:
        w_in[d] = begin(w_hbm[slot[d]], wv.at[slot[d]])
        x_in[d] = begin(x_hbm.at[d], xv.at[d])
    ct_in = begin(ct_hbm, ctv)

    acc_in.wait()
    gu, dh = acc[:, : 2 * units], acc[:, 2 * units :]
    for d in (3, 5):
        w_in[d].wait()
        x_in[d].wait()
        c_in[d].wait()
        down_in[d].wait()
        gu = gu + jnp.dot(xv[d], wv[slot[d]], preferred_element_type=F32)
        dh = dh + jnp.dot(cv[d - 3], dwv[(d - 3) // 2], preferred_element_type=F32)
    x_in[4].wait()
    c_in[4].wait()
    gu = gu + jnp.dot(xv[4], gu4_ref[...], preferred_element_type=F32)
    dh = dh + jnp.dot(cv[1], down4_ref[...], preferred_element_type=F32)
    gate, up = gu[:, :units], gu[:, units:]
    dh = 0.5 * dh
    sig = jax.nn.sigmoid(gate)
    act = gate * sig
    hidden = (act * up).astype(BF16)
    d_gate = (dh * up * sig * (1.0 + gate * (1.0 - sig))).astype(BF16)
    d_up = (dh * act).astype(BF16)
    both = jnp.concatenate([d_gate, d_up], axis=1)
    out_copies = []
    sums = {}
    for d in (4, 3, 5) + EARLY:
        if d in EARLY:
            w_in[d].wait()
            x_in[d].wait()
        w = gu4_ref[...] if d == 4 else wv[slot[d]]
        out = lax.dot_general(both, w, (((1,), (1,)), ((), ())), preferred_element_type=F32)
        terms = jnp.sum(xv[d].astype(F32) * out, axis=0, keepdims=True)
        sums[d] = terms / gain_ref[d]
        out = out.astype(BF16)
        for k in range(2 * nx):
            ov[k, d] = out[k * part : (k + 1) * part]
        out_copies.append(begin(ov.at[pl.ds(nx, nx), d], other_hbm.at[:, d]))
        out_copies.append(begin(ov.at[pl.ds(0, nx), d], mine_hbm.at[:, d]))
    ct_in.wait()
    for d in range(nz):
        res = jnp.dot(ctv[d], hidden, preferred_element_type=F32)
        res = (0.5 * res).astype(BF16)
        high = sums[d].astype(BF16)
        left = sums[d] - high.astype(F32)
        mid = left.astype(BF16)
        low = (left - mid.astype(F32)).astype(BF16)
        extra = jnp.concatenate([high, mid, low, jnp.zeros((5, cols), BF16)], axis=0)
        extra = jnp.concatenate([extra, jnp.zeros((8, units - cols), BF16)], axis=1)
        for y in range(ny):
            dv[y, d, :rows] = res[y * rows : (y + 1) * rows]
            dv[y, d, rows:] = extra
        out_copies.append(begin(dv.at[:, d], dd_hbm.at[:, d]))
    for copy in out_copies:
        copy.wait()


def rows_kernel(at_ref, got_ref, out_ref):
    ny, nz, longer, _ = got_ref.shape
    rows = longer - 8
    half = rows // 2
    sums = []
    for d in range(nz):
        total = got_ref[0, d].astype(F32)
        for k in range(1, ny):
            total = total + got_ref[k, d].astype(F32)
        part = total[:rows].astype(BF16)
        to = (at_ref[0] + d) % nz
        out_ref[to, :half] = part[:half]
        out_ref[nz + to, :half] = part[half:]
        sums.append(jnp.sum(total[rows:], axis=0, keepdims=True))
    extra = jnp.concatenate(sums, axis=0)
    extra = pltpu.roll(extra, at_ref[0], 0).astype(BF16)
    for k in range(2 * nz):
        out_ref[k, half:] = extra


def ring_kernel(got_ref, out_ref, sum_ref):
    half = out_ref.shape[0]
    cols = sum_ref.shape[2]
    total = got_ref[0].astype(F32)
    for k in range(1, got_ref.shape[0]):
        total = total + got_ref[k].astype(F32)
    out_ref[...] = total[:half]
    for k in range(sum_ref.shape[0]):
        sum_ref[k] = total[half:, :cols]


def chip_kernel(mine_ref, theirs_ref, *out_refs):
    for k, out_ref in enumerate(out_refs):
        out_ref[...] = (mine_ref[k].astype(F32) + theirs_ref[k].astype(F32)).astype(BF16)


def finish_kernel(at_ref, got0, got1, got2, got3, x_ref, c_ref, gain_ref, out_ref, dn_ref):
    nz, _, cols = got0.shape
    for d in range(nz):
        own = pl.ds(pl.multiple_of(((at_ref[0] + d) % nz) * cols, cols), cols)
        total = got0[d].astype(F32)
        for got in (got1, got2, got3):
            total = total + got[d].astype(F32)
        dn_ref[:, own] = total.astype(BF16)
    v = x_ref[...].astype(F32)
    inv = lax.rsqrt(jnp.mean(v * v, axis=-1, keepdims=True) + EPS)
    xhat = v * inv
    dn = dn_ref[...].astype(F32)
    gs = gain_ref[...] * dn
    m = jnp.mean(gs * xhat, axis=-1, keepdims=True)
    out_ref[...] = (c_ref[...].astype(F32) + inv * (gs - xhat * m)).astype(BF16)


def place_kernel(at_ref, p0, p1, p2, p3, other_ref, out_ref):
    n = 4
    part = out_ref.shape[0] // (2 * n)
    for k, piece in enumerate((p0, p1, p2, p3)):
        spot = (at_ref[2] + k) % n
        own = pl.multiple_of((at_ref[1] * n + spot) * part, part)
        far = pl.multiple_of(((1 - at_ref[1]) * n + spot) * part, part)
        out_ref[pl.ds(own, part), :] = piece[:part]
        out_ref[pl.ds(far, part), :] = other_ref[k, :part]


def near(*arrays):
    return [pltpu.with_memory_space_constraint(a, pltpu.VMEM) for a in arrays]


def vmem(n):
    return [pl.BlockSpec(memory_space=pltpu.VMEM)] * n


def work(inputs, gain, gate_weight, up_weight, down_weight, cotangent):
    nz, ny, nx = lax.axis_size("fs_0"), lax.axis_size("fs_1"), lax.axis_size("x")
    rep, zl = lax.axis_index("rep"), lax.axis_index("fs_0")
    x, c = lax.axis_index("x"), lax.axis_index("c")
    tokens, width = inputs.shape
    rows, units = gate_weight.shape
    cols = width // nz
    part = tokens // 2 // nx
    gain2 = gain[None]
    at = jnp.stack([zl, c, x]).astype(jnp.int32)

    def relay(own):
        fwd, bwd = [own], [own]
        for _ in range(3):
            fwd.append(shifted(fwd[-1], RING, 1))
            bwd.append(shifted(bwd[-1], RING, -1))
        return fwd, bwd

    gu0 = from_all(jnp.concatenate([gate_weight, up_weight], axis=1), "fs_1")
    down0 = from_all(down_weight, "fs_1")
    gu_f, gu_b = relay(gu0.reshape(ny * rows, 2 * units))
    down_f, down_b = relay(down0.reshape(ny * rows, units))
    gu4 = shifted(gu_f[3], RING, 1)
    down4 = shifted(down_b[3], RING, -1)

    def spot(i, at):
        return ((i // nx + at[1]) % 2) * nx + (i + at[2]) % nx

    xr = pl.pallas_call(
        prepare_tokens,
        out_shape=jax.ShapeDtypeStruct((nz, tokens, cols), BF16),
        grid_spec=pltpu.PrefetchScalarGridSpec(
            num_scalar_prefetch=1,
            grid=(2 * nx,),
            in_specs=[
                pl.BlockSpec((part, width), lambda i, at: (spot(i, at), 0)),
                pl.BlockSpec((1, width), lambda i, at: (0, 0)),
            ],
            out_specs=pl.BlockSpec((nz, part, cols), lambda i, at: (0, i, 0)),
        ),
        name="prepare_x",
    )(at, inputs, gain2)
    cr, ct = pl.pallas_call(
        prepare_cotangent,
        out_shape=(
            jax.ShapeDtypeStruct((nz, tokens, cols), BF16),
            jax.ShapeDtypeStruct((nz, cols, tokens), BF16),
        ),
        grid_spec=pltpu.PrefetchScalarGridSpec(
            num_scalar_prefetch=1,
            grid=(nx,),
            in_specs=[
                pl.BlockSpec((part, width), lambda i, at: (spot(2 * i, at), 0)),
                pl.BlockSpec((part, width), lambda i, at: (spot(2 * i + 1, at), 0)),
            ],
            out_specs=(
                pl.BlockSpec((nz, 2 * part, cols), lambda i, at: (0, i, 0)),
                pl.BlockSpec((nz, cols, 2 * part), lambda i, at: (0, 0, i)),
            ),
        ),
        name="prepare_c",
    )(at, cotangent, cotangent)

    gain_ring = rolled(gain.reshape(nz, 1, cols), zl)
    acc = pl.pallas_call(
        forward_kernel,
        out_shape=jax.ShapeDtypeStruct((tokens, 3 * units), F32),
        in_specs=vmem(12),
        out_specs=pl.BlockSpec(memory_space=pltpu.VMEM),
        name="forward",
    )(
        *(xr, cr, gu_f[0], gu_b[1], gu_f[1], gu_b[2], gu_f[2]),
        *(down_f[0], down_b[1], down_f[1], down_b[2], down_f[2]),
    )
    anywhere = pl.BlockSpec(memory_space=pl.ANY)
    mine, other, dd = pl.pallas_call(
        grad_kernel,
        out_shape=(
            jax.ShapeDtypeStruct((nx, nz, part, cols), BF16),
            jax.ShapeDtypeStruct((nx, nz, part, cols), BF16),
            jax.ShapeDtypeStruct((ny, nz, rows + 8, units), BF16),
        ),
        in_specs=vmem(3) + [anywhere] * 13,
        out_specs=(anywhere,) * 3,
        scratch_shapes=[
            pltpu.VMEM((tokens, 3 * units), F32),
            pltpu.VMEM((nz, tokens, cols), BF16),
            pltpu.VMEM((3, tokens, cols), BF16),
            pltpu.VMEM((nz, cols, tokens), BF16),
            pltpu.VMEM((7, cols, 2 * units), BF16),
            pltpu.VMEM((2, cols, units), BF16),
            pltpu.VMEM((2 * nx, nz, part, cols), BF16),
            pltpu.VMEM((ny, nz, rows + 8, units), BF16),
            pltpu.SemaphoreType.DMA((48,)),
        ],
        name="grad",
    )(
        *(gain_ring, *near(gu4, down4), acc, xr, cr, ct),
        *(gu_f[0], gu_b[1], gu_b[2], gu_b[3], gu_f[3], gu_f[2], gu_f[1], down_b[3], down_f[3]),
    )
    theirs = shifted(other, "c", 1)
    dy = exchanged(dd, "fs_1")

    chunk = jax.ShapeDtypeStruct((nz, part, cols), BF16)
    chip = pl.pallas_call(
        chip_kernel,
        out_shape=(chunk,) * 4,
        in_specs=vmem(2),
        out_specs=tuple(vmem(4)),
        name="chip",
    )(mine, *near(theirs))
    got = [chip[0]]
    for k in (1, 2, 3):
        got.append(shifted(chip[k], "x", k))
    own = pl.BlockSpec((part, width), lambda i, at: (at[1] * nx + at[2], 0))
    ig = pl.pallas_call(
        finish_kernel,
        out_shape=jax.ShapeDtypeStruct((part, width), BF16),
        grid_spec=pltpu.PrefetchScalarGridSpec(
            num_scalar_prefetch=1,
            grid=(1,),
            in_specs=vmem(4) + [own, own, pl.BlockSpec((1, width), lambda i, at: (0, 0))],
            out_specs=pl.BlockSpec((part, width), lambda i, at: (0, 0)),
            scratch_shapes=[pltpu.VMEM((part, width), BF16)],
        ),
        name="finish",
    )(at, got[0], *near(*got[1:]), inputs, cotangent, gain2)
    pieces = [ig]
    for k in (1, 2, 3):
        pieces.append(shifted(ig, "x", -k))
    ig_other = shifted(jnp.stack(pieces), "c", 1)
    out = pl.pallas_call(
        place_kernel,
        out_shape=jax.ShapeDtypeStruct((tokens, width), BF16),
        in_specs=[pl.BlockSpec(memory_space=pltpu.SMEM)] + vmem(5),
        out_specs=pl.BlockSpec(memory_space=pltpu.VMEM),
        name="place",
    )(at, pieces[0], *near(*pieces[1:], ig_other))

    dz = pl.pallas_call(
        rows_kernel,
        out_shape=jax.ShapeDtypeStruct((2 * nz, rows // 2 + 8, units), BF16),
        in_specs=[pl.BlockSpec(memory_space=pltpu.SMEM)] + vmem(1),
        out_specs=pl.BlockSpec(memory_space=pltpu.VMEM),
        name="ysum",
    )(at, *near(dy))
    dz = exchanged(dz, RING)
    own, gain_own = pl.pallas_call(
        ring_kernel,
        out_shape=(
            jax.ShapeDtypeStruct((rows // 2, units), F32),
            jax.ShapeDtypeStruct((lax.axis_size(TP), nz, cols), F32),
        ),
        in_specs=vmem(1),
        out_specs=tuple(vmem(2)),
        name="zsum",
    )(*near(dz))
    gain_all = exchanged(gain_own, TP)
    gain_gradient = jnp.sum(gain_all, axis=0).reshape(width)
    far = shifted(own, "rep", 1)
    pair = rolled(jnp.stack([own, far]), rep)
    d_down = pair.reshape(rows, units)
    return (out, gain_gradient, d_down)


def solution(mesh):
    torus = Mesh(
        mesh.devices.reshape(mesh.shape["rep"], 8, 4, 4, 2),
        ("rep", "fs_0", "fs_1", "x", "c"),
    )
    return jax.shard_map(
        work,
        mesh=torus,
        in_specs=(P(REP_FS, None), P(), P(FS, TP), P(FS, TP), P(FS, TP), P(REP_FS, None)),
        out_specs=(P(REP_FS, None), P(), P(FS, TP)),
        check_vma=False,
    )
```

```python
import jax
import jax.numpy as jnp
from jax import lax
from jax.experimental import pallas as pl
from jax.experimental.pallas import tpu as pltpu
from jax.sharding import Mesh
from jax.sharding import PartitionSpec as P

FS = ("fs_0", "fs_1")
REP_FS = ("rep", "fs_0", "fs_1")
TP = ("x", "c")
RING = ("rep", "fs_0")
PLANE = ("fs_1", "x", "c")
EPS = 1e-06
EARLY = (0, 1, 7, 2, 6)
F32 = jnp.float32
BF16 = jnp.bfloat16


def shifted(v, axis, by):
    n = lax.axis_size(axis)
    return lax.ppermute(v, axis, [(i, (i + by) % n) for i in range(n)])


def exchanged(v, axis):
    return lax.all_to_all(v, axis, 0, 0, tiled=True)


def from_all(v, axis):
    n = lax.axis_size(axis)
    return exchanged(jnp.broadcast_to(v[None], (n, *v.shape)), axis)


def rolled(v, start):
    return lax.dynamic_slice_in_dim(jnp.concatenate([v, v], axis=0), start, v.shape[0], axis=0)


def prepare_tokens(at_ref, x_ref, gain_ref, out_ref):
    nz, _, cols = out_ref.shape
    v = x_ref[...].astype(F32)
    inv = lax.rsqrt(jnp.mean(v * v, axis=-1, keepdims=True) + EPS)
    for d in range(nz):
        own = pl.ds(pl.multiple_of(((at_ref[0] + d) % nz) * cols, cols), cols)
        part = x_ref[:, own].astype(F32)
        out_ref[d] = (part * inv * gain_ref[:, own]).astype(BF16)


def prepare_cotangent(at_ref, lo_ref, hi_ref, out_ref, turned_ref):
    nz, _, cols = out_ref.shape
    for d in range(nz):
        own = pl.ds(pl.multiple_of(((at_ref[0] + d) % nz) * cols, cols), cols)
        part = jnp.concatenate([lo_ref[:, own], hi_ref[:, own]], axis=0)
        out_ref[d] = part
        turned_ref[d] = part.T


def forward_kernel(x_ref, c_ref, *refs):
    w_refs, acc_ref = refs[:-1], refs[-1]
    units = acc_ref.shape[1] // 3
    gu = dh = None
    for d, w in zip(EARLY, w_refs):
        a = jnp.dot(x_ref[d], w[:, : 2 * units], preferred_element_type=F32)
        b = jnp.dot(c_ref[d], w[:, 2 * units :], preferred_element_type=F32)
        gu = a if gu is None else gu + a
        dh = b if dh is None else dh + b
    acc_ref[:, : 2 * units] = gu
    acc_ref[:, 2 * units :] = dh


def starter(sems):
    used = [0]

    def begin(src, dst):
        copy = pltpu.make_async_copy(src, dst, sems.at[used[0]])
        used[0] += 1
        copy.start()
        return copy

    return begin


def down_kernel(lo_ref, hi_ref, acc_hbm, x_hbm, c_hbm, ct_hbm, w3_hbm, w5_hbm, *refs):
    dd_hbm, both_ref, acc, xv, cv, ctv, wv, dv, sems = refs
    units = acc.shape[1] // 3
    ny, nz, rows, _ = dv.shape
    cols = xv.shape[2]
    begin = starter(sems)
    acc_in = begin(acc_hbm, acc)
    loads = []
    for i, w_hbm in enumerate((w3_hbm, w5_hbm)):
        d = 3 + 2 * i
        loads.append(
            (
                begin(w_hbm, wv.at[i]),
                begin(x_hbm.at[d], xv.at[2 * i]),
                begin(c_hbm.at[d], cv.at[2 * i]),
            )
        )
    mid_in = (begin(x_hbm.at[4], xv.at[1]), begin(c_hbm.at[4], cv.at[1]))
    ct_in = begin(ct_hbm, ctv)
    acc_in.wait()
    gu, dh = acc[:, : 2 * units], acc[:, 2 * units :]
    for i in range(2):
        for copy in loads[i]:
            copy.wait()
        gu = gu + jnp.dot(xv[2 * i], wv[i, :, : 2 * units], preferred_element_type=F32)
        dh = dh + jnp.dot(cv[2 * i], wv[i, :, 2 * units :], preferred_element_type=F32)
    for copy in mid_in:
        copy.wait()
    half = cols // 2
    for w, at in ((lo_ref, slice(0, half)), (hi_ref, slice(half, cols))):
        gu = gu + jnp.dot(xv[1, :, at], w[:, : 2 * units], preferred_element_type=F32)
        dh = dh + jnp.dot(cv[1, :, at], w[:, 2 * units :], preferred_element_type=F32)
    gate, up = gu[:, :units], gu[:, units:]
    dh = 0.5 * dh
    sig = jax.nn.sigmoid(gate)
    act = gate * sig
    hidden = (act * up).astype(BF16)
    both_ref[:, :units] = (dh * up * sig * (1.0 + gate * (1.0 - sig))).astype(BF16)
    both_ref[:, units:] = (dh * act).astype(BF16)
    ct_in.wait()
    out_copies = []
    for d in range(nz):
        res = jnp.dot(ctv[d], hidden, preferred_element_type=F32)
        res = (0.5 * res).astype(BF16)
        for y in range(ny):
            dv[y, d] = res[y * rows : (y + 1) * rows]
        out_copies.append(begin(dv.at[:, d], dd_hbm.at[:, d]))
    for copy in out_copies:
        copy.wait()


def grad_kernel(gain_ref, lo_ref, hi_ref, both_ref, x_hbm, *refs):
    w_hbm, (mine_hbm, other_hbm, sum_ref) = refs[:7], refs[7:10]
    xv, wv, ov, sems = refs[10:]
    _, _, cols = xv.shape
    nx, part = mine_hbm.shape[0], mine_hbm.shape[2]
    units = both_ref.shape[1] // 2
    begin = starter(sems)
    slot = {0: 0, 1: 1, 2: 2, 3: 3, 5: 4, 6: 5, 7: 6}
    x_in, w_in = {}, {}
    for d in (4, 3, 5) + EARLY:
        x_in[d] = begin(x_hbm.at[d], xv.at[d])
        if d != 4:
            w_in[d] = begin(w_hbm[slot[d]], wv.at[slot[d]])
    half = cols // 2
    halves = ((lo_ref, slice(0, half)), (hi_ref, slice(half, cols)))
    both = both_ref[...]
    out_copies = []
    for d in (4, 3, 5) + EARLY:
        if d != 4:
            w_in[d].wait()
        x_in[d].wait()
        pieces = halves if d == 4 else ((wv.at[slot[d]], slice(0, cols)),)
        for w, at in pieces:
            out = lax.dot_general(
                both, w[:, : 2 * units], (((1,), (1,)), ((), ())), preferred_element_type=F32
            )
            terms = jnp.sum(xv[d, :, at].astype(F32) * out, axis=0, keepdims=True)
            sum_ref[d, :, at] = terms / gain_ref[d, :, at]
            out = out.astype(BF16)
            for k in range(2 * nx):
                ov[k, d, :, at] = out[k * part : (k + 1) * part]
        out_copies.append(begin(ov.at[pl.ds(nx, nx), d], other_hbm.at[:, d]))
        out_copies.append(begin(ov.at[pl.ds(0, nx), d], mine_hbm.at[:, d]))
    for copy in out_copies:
        copy.wait()


def rows_kernel(at_ref, own_ref, got_ref, out_ref):
    ny, nz, rows, units = got_ref.shape
    half = rows // 2
    cols = own_ref.shape[2]
    for d in range(nz):
        total = got_ref[0, d].astype(F32)
        for k in range(1, ny):
            total = total + got_ref[k, d].astype(F32)
        part = total.astype(BF16)
        to = (at_ref[0] + d) % nz
        out_ref[to, :half] = part[:half]
        out_ref[nz + to, :half] = part[half:]
    extra = jnp.concatenate([own_ref[d] for d in range(nz)], axis=0)
    extra = pltpu.roll(extra, at_ref[0], 0).astype(BF16)
    extra = jnp.concatenate([extra, jnp.zeros((nz, units - cols), BF16)], axis=1)
    for k in range(2 * nz):
        out_ref[k, half:] = extra


def ring_kernel(got_ref, out_ref, sum_ref):
    half = out_ref.shape[0]
    cols = sum_ref.shape[2]
    total = got_ref[0].astype(F32)
    for k in range(1, got_ref.shape[0]):
        total = total + got_ref[k].astype(F32)
    out_ref[...] = total[:half]
    for k in range(sum_ref.shape[0]):
        sum_ref[k] = total[half:, :cols]


def chip_kernel(mine_ref, theirs_ref, *out_refs):
    for k, out_ref in enumerate(out_refs):
        out_ref[...] = (mine_ref[k].astype(F32) + theirs_ref[k].astype(F32)).astype(BF16)


def finish_kernel(at_ref, got0, got1, got2, got3, x_ref, c_ref, gain_ref, out_ref, dn_ref):
    nz, _, cols = got0.shape
    for d in range(nz):
        own = pl.ds(pl.multiple_of(((at_ref[0] + d) % nz) * cols, cols), cols)
        total = got0[d].astype(F32)
        for got in (got1, got2, got3):
            total = total + got[d].astype(F32)
        dn_ref[:, own] = total.astype(BF16)
    v = x_ref[...].astype(F32)
    inv = lax.rsqrt(jnp.mean(v * v, axis=-1, keepdims=True) + EPS)
    xhat = v * inv
    dn = dn_ref[...].astype(F32)
    gs = gain_ref[...] * dn
    m = jnp.mean(gs * xhat, axis=-1, keepdims=True)
    out_ref[...] = (c_ref[...].astype(F32) + inv * (gs - xhat * m)).astype(BF16)


def place_kernel(at_ref, p0, p1, p2, p3, other_ref, out_ref):
    n = 4
    part = out_ref.shape[0] // (2 * n)
    for k, piece in enumerate((p0, p1, p2, p3)):
        spot = (at_ref[2] + k) % n
        own = pl.multiple_of((at_ref[1] * n + spot) * part, part)
        far = pl.multiple_of(((1 - at_ref[1]) * n + spot) * part, part)
        out_ref[pl.ds(own, part), :] = piece[:part]
        out_ref[pl.ds(far, part), :] = other_ref[k, :part]


def near(*arrays):
    return [pltpu.with_memory_space_constraint(a, pltpu.VMEM) for a in arrays]


def vmem(n):
    return [pl.BlockSpec(memory_space=pltpu.VMEM)] * n


def work(inputs, gain, gate_weight, up_weight, down_weight, cotangent):
    nz, ny, nx = lax.axis_size("fs_0"), lax.axis_size("fs_1"), lax.axis_size("x")
    rep, zl = lax.axis_index("rep"), lax.axis_index("fs_0")
    x, c = lax.axis_index("x"), lax.axis_index("c")
    tokens, width = inputs.shape
    rows, units = gate_weight.shape
    cols = width // nz
    part = tokens // 2 // nx
    gain2 = gain[None]
    at = jnp.stack([zl, c, x]).astype(jnp.int32)

    w = jnp.concatenate([gate_weight, up_weight, down_weight], axis=1)
    w0 = from_all(w, "fs_1").reshape(ny * rows, 3 * units)
    fwd, bwd = [w0], [w0]
    for _ in range(3):
        fwd.append(shifted(fwd[-1], RING, 1))
        bwd.append(shifted(bwd[-1], RING, -1))
    mid = cols // 2
    last_f = shifted(fwd[-1][:mid], RING, 1)
    last_b = shifted(bwd[-1][mid:], RING, -1)
    weights = [w0, bwd[1], bwd[2], bwd[3], fwd[3], fwd[2], fwd[1]]

    def spot(i, at):
        return ((i // nx + at[1]) % 2) * nx + (i + at[2]) % nx

    xr = pl.pallas_call(
        prepare_tokens,
        out_shape=jax.ShapeDtypeStruct((nz, tokens, cols), BF16),
        grid_spec=pltpu.PrefetchScalarGridSpec(
            num_scalar_prefetch=1,
            grid=(2 * nx,),
            in_specs=[
                pl.BlockSpec((part, width), lambda i, at: (spot(i, at), 0)),
                pl.BlockSpec((1, width), lambda i, at: (0, 0)),
            ],
            out_specs=pl.BlockSpec((nz, part, cols), lambda i, at: (0, i, 0)),
        ),
        name="prepare_x",
    )(at, inputs, gain2)
    cr, ct = pl.pallas_call(
        prepare_cotangent,
        out_shape=(
            jax.ShapeDtypeStruct((nz, tokens, cols), BF16),
            jax.ShapeDtypeStruct((nz, cols, tokens), BF16),
        ),
        grid_spec=pltpu.PrefetchScalarGridSpec(
            num_scalar_prefetch=1,
            grid=(nx,),
            in_specs=[
                pl.BlockSpec((part, width), lambda i, at: (spot(2 * i, at), 0)),
                pl.BlockSpec((part, width), lambda i, at: (spot(2 * i + 1, at), 0)),
            ],
            out_specs=(
                pl.BlockSpec((nz, 2 * part, cols), lambda i, at: (0, i, 0)),
                pl.BlockSpec((nz, cols, 2 * part), lambda i, at: (0, 0, i)),
            ),
        ),
        name="prepare_c",
    )(at, cotangent, cotangent)

    gain_ring = rolled(gain.reshape(nz, 1, cols), zl)
    acc = pl.pallas_call(
        forward_kernel,
        out_shape=jax.ShapeDtypeStruct((tokens, 3 * units), F32),
        in_specs=vmem(7),
        out_specs=pl.BlockSpec(memory_space=pltpu.VMEM),
        name="forward",
    )(xr, cr, w0, bwd[1], fwd[1], bwd[2], fwd[2])
    anywhere = pl.BlockSpec(memory_space=pl.ANY)
    dd, both = pl.pallas_call(
        down_kernel,
        out_shape=(
            jax.ShapeDtypeStruct((ny, nz, rows, units), BF16),
            jax.ShapeDtypeStruct((tokens, 2 * units), BF16),
        ),
        in_specs=vmem(2) + [anywhere] * 6,
        out_specs=(anywhere, pl.BlockSpec(memory_space=pltpu.VMEM)),
        scratch_shapes=[
            pltpu.VMEM((tokens, 3 * units), F32),
            pltpu.VMEM((3, tokens, cols), BF16),
            pltpu.VMEM((3, tokens, cols), BF16),
            pltpu.VMEM((nz, cols, tokens), BF16),
            pltpu.VMEM((2, cols, 3 * units), BF16),
            pltpu.VMEM((ny, nz, rows, units), BF16),
            pltpu.SemaphoreType.DMA((24,)),
        ],
        name="down",
    )(*near(last_f, last_b), acc, xr, cr, ct, bwd[3], fwd[3])
    dy = exchanged(dd, "fs_1")
    mine, other, sums = pl.pallas_call(
        grad_kernel,
        out_shape=(
            jax.ShapeDtypeStruct((nx, nz, part, cols), BF16),
            jax.ShapeDtypeStruct((nx, nz, part, cols), BF16),
            jax.ShapeDtypeStruct((nz, 1, cols), F32),
        ),
        in_specs=vmem(4) + [anywhere] * 8,
        out_specs=(anywhere, anywhere, pl.BlockSpec(memory_space=pltpu.VMEM)),
        scratch_shapes=[
            pltpu.VMEM((nz, tokens, cols), BF16),
            pltpu.VMEM((7, cols, 3 * units), BF16),
            pltpu.VMEM((2 * nx, nz, part, cols), BF16),
            pltpu.SemaphoreType.DMA((32,)),
        ],
        name="grad",
    )(gain_ring, *near(last_f, last_b), both, xr, *weights)
    theirs = shifted(other, "c", 1)
    chunk = jax.ShapeDtypeStruct((nz, part, cols), BF16)
    chip = pl.pallas_call(
        chip_kernel,
        out_shape=(chunk,) * 4,
        in_specs=vmem(2),
        out_specs=tuple(vmem(4)),
        compiler_params=pltpu.CompilerParams(vmem_limit_bytes=32 << 20),
        name="chip",
    )(mine, *near(theirs))
    got = [chip[0]]
    for k in (1, 2, 3):
        got.append(shifted(chip[k], "x", k))
    own = pl.BlockSpec((part, width), lambda i, at: (at[1] * nx + at[2], 0))
    ig = pl.pallas_call(
        finish_kernel,
        out_shape=jax.ShapeDtypeStruct((part, width), BF16),
        grid_spec=pltpu.PrefetchScalarGridSpec(
            num_scalar_prefetch=1,
            grid=(1,),
            in_specs=vmem(4) + [own, own, pl.BlockSpec((1, width), lambda i, at: (0, 0))],
            out_specs=pl.BlockSpec((part, width), lambda i, at: (0, 0)),
            scratch_shapes=[pltpu.VMEM((part, width), BF16)],
        ),
        name="finish",
    )(at, got[0], *near(*got[1:]), inputs, cotangent, gain2)
    pieces = [ig]
    for k in (1, 2, 3):
        pieces.append(shifted(ig, "x", -k))
    ig_other = shifted(jnp.stack(pieces), "c", 1)
    out = pl.pallas_call(
        place_kernel,
        out_shape=jax.ShapeDtypeStruct((tokens, width), BF16),
        in_specs=[pl.BlockSpec(memory_space=pltpu.SMEM)] + vmem(5),
        out_specs=pl.BlockSpec(memory_space=pltpu.VMEM),
        name="place",
    )(at, pieces[0], *near(*pieces[1:], ig_other))

    dz = pl.pallas_call(
        rows_kernel,
        out_shape=jax.ShapeDtypeStruct((2 * nz, rows // 2 + 8, units), BF16),
        in_specs=[pl.BlockSpec(memory_space=pltpu.SMEM)] + vmem(2),
        out_specs=pl.BlockSpec(memory_space=pltpu.VMEM),
        name="ysum",
    )(at, sums, *near(dy))
    dz = exchanged(dz, RING)
    own, gain_own = pl.pallas_call(
        ring_kernel,
        out_shape=(
            jax.ShapeDtypeStruct((rows // 2, units), F32),
            jax.ShapeDtypeStruct((lax.axis_size(PLANE), nz, cols), F32),
        ),
        in_specs=vmem(1),
        out_specs=tuple(vmem(2)),
        name="zsum",
    )(*near(dz))
    gain_all = exchanged(gain_own, PLANE)
    gain_gradient = jnp.sum(gain_all, axis=0).reshape(width)
    far = shifted(own, "rep", 1)
    pair = rolled(jnp.stack([own, far]), rep)
    d_down = pair.reshape(rows, units)
    return (out, gain_gradient, d_down)


def solution(mesh):
    torus = Mesh(
        mesh.devices.reshape(mesh.shape["rep"], 8, 4, 4, 2),
        ("rep", "fs_0", "fs_1", "x", "c"),
    )
    return jax.shard_map(
        work,
        mesh=torus,
        in_specs=(P(REP_FS, None), P(), P(FS, TP), P(FS, TP), P(FS, TP), P(REP_FS, None)),
        out_specs=(P(REP_FS, None), P(), P(FS, TP)),
        check_vma=False,
    )
```

```python
import jax
import jax.numpy as jnp
from jax import lax
from jax.experimental import pallas as pl
from jax.experimental.pallas import tpu as pltpu
from jax.sharding import Mesh
from jax.sharding import PartitionSpec as P

FS = ("fs_0", "fs_1")
REP_FS = ("rep", "fs_0", "fs_1")
TP = ("x", "c")
RING = ("rep", "fs_0")
EPS = 1e-06
EARLY = (0, 1, 7, 2, 6)
F32 = jnp.float32
BF16 = jnp.bfloat16


def shifted(v, axis, by):
    n = lax.axis_size(axis)
    return lax.ppermute(v, axis, [(i, (i + by) % n) for i in range(n)])


def exchanged(v, axis):
    return lax.all_to_all(v, axis, 0, 0, tiled=True)


def from_all(v, axis):
    n = lax.axis_size(axis)
    return exchanged(jnp.broadcast_to(v[None], (n, *v.shape)), axis)


def rolled(v, start):
    return lax.dynamic_slice_in_dim(jnp.concatenate([v, v], axis=0), start, v.shape[0], axis=0)


def prepare_tokens(at_ref, x_ref, gain_ref, out_ref):
    nz, _, cols = out_ref.shape
    v = x_ref[...].astype(F32)
    inv = lax.rsqrt(jnp.mean(v * v, axis=-1, keepdims=True) + EPS)
    for d in range(nz):
        own = pl.ds(pl.multiple_of(((at_ref[0] + d) % nz) * cols, cols), cols)
        part = x_ref[:, own].astype(F32)
        out_ref[d] = (part * inv * gain_ref[:, own]).astype(BF16)


def prepare_cotangent(at_ref, lo_ref, hi_ref, out_ref, turned_ref):
    nz, _, cols = out_ref.shape
    for d in range(nz):
        own = pl.ds(pl.multiple_of(((at_ref[0] + d) % nz) * cols, cols), cols)
        part = jnp.concatenate([lo_ref[:, own], hi_ref[:, own]], axis=0)
        out_ref[d] = part
        turned_ref[d] = part.T


def forward_kernel(x_ref, c_ref, *refs):
    w_refs, acc_ref = refs[:-1], refs[-1]
    units = acc_ref.shape[1] // 3
    gu = dh = None
    for d, w in zip(EARLY, w_refs):
        a = jnp.dot(x_ref[d], w[:, : 2 * units], preferred_element_type=F32)
        b = jnp.dot(c_ref[d], w[:, 2 * units :], preferred_element_type=F32)
        gu = a if gu is None else gu + a
        dh = b if dh is None else dh + b
    acc_ref[:, : 2 * units] = gu
    acc_ref[:, 2 * units :] = dh


def grad_kernel(gain_ref, lo_ref, hi_ref, acc_hbm, x_hbm, c_hbm, ct_hbm, *refs):
    w_hbm, (mine_hbm, other_hbm, dd_hbm) = refs[:7], refs[7:10]
    acc, xv, cv, ctv, wv, ov, dv, sems = refs[10:]
    units = acc.shape[1] // 3
    nz, _, cols = xv.shape
    ny, _, longer, _ = dv.shape
    nx, part = mine_hbm.shape[0], mine_hbm.shape[2]
    rows = longer - 8
    used = [0]

    def begin(src, dst):
        copy = pltpu.make_async_copy(src, dst, sems.at[used[0]])
        used[0] += 1
        copy.start()
        return copy

    slot = {0: 0, 1: 1, 2: 2, 3: 3, 5: 4, 6: 5, 7: 6}
    acc_in = begin(acc_hbm, acc)
    x_in, c_in, w_in = {}, {}, {}
    for d in (3, 5):
        w_in[d] = begin(w_hbm[slot[d]], wv.at[slot[d]])
        x_in[d] = begin(x_hbm.at[d], xv.at[d])
        c_in[d] = begin(c_hbm.at[d], cv.at[d - 3])
    x_in[4] = begin(x_hbm.at[4], xv.at[4])
    c_in[4] = begin(c_hbm.at[4], cv.at[1])

    half = cols // 2
    halves = ((lo_ref, slice(0, half)), (hi_ref, slice(half, cols)))
    acc_in.wait()
    gu, dh = acc[:, : 2 * units], acc[:, 2 * units :]
    for d in (3, 5):
        w_in[d].wait()
        x_in[d].wait()
        c_in[d].wait()
        for e in EARLY if d == 3 else ():
            w_in[e] = begin(w_hbm[slot[e]], wv.at[slot[e]])
            x_in[e] = begin(x_hbm.at[e], xv.at[e])
        w = wv.at[slot[d]]
        gu = gu + jnp.dot(xv[d], w[:, : 2 * units], preferred_element_type=F32)
        dh = dh + jnp.dot(cv[d - 3], w[:, 2 * units :], preferred_element_type=F32)
    x_in[4].wait()
    c_in[4].wait()
    for w, at in halves:
        gu = gu + jnp.dot(xv[4, :, at], w[:, : 2 * units], preferred_element_type=F32)
        dh = dh + jnp.dot(cv[1, :, at], w[:, 2 * units :], preferred_element_type=F32)
    gate, up = gu[:, :units], gu[:, units:]
    dh = 0.5 * dh
    sig = jax.nn.sigmoid(gate)
    act = gate * sig
    hidden = (act * up).astype(BF16)
    d_gate = (dh * up * sig * (1.0 + gate * (1.0 - sig))).astype(BF16)
    d_up = (dh * act).astype(BF16)
    both = jnp.concatenate([d_gate, d_up], axis=1)
    ct_in = begin(ct_hbm, ctv)
    out_copies = []
    sums = {}
    for d in (4, 3, 5) + EARLY:
        if d in EARLY:
            w_in[d].wait()
            x_in[d].wait()
        pieces = halves if d == 4 else ((wv.at[slot[d]], slice(0, cols)),)
        got = []
        for w, at in pieces:
            out = lax.dot_general(
                both, w[:, : 2 * units], (((1,), (1,)), ((), ())), preferred_element_type=F32
            )
            terms = jnp.sum(xv[d, :, at].astype(F32) * out, axis=0, keepdims=True)
            got.append(terms / gain_ref[d, :, at])
            out = out.astype(BF16)
            for k in range(2 * nx):
                ov[k, d, :, at] = out[k * part : (k + 1) * part]
        sums[d] = got[0] if len(got) == 1 else jnp.concatenate(got, axis=1)
        out_copies.append(begin(ov.at[pl.ds(nx, nx), d], other_hbm.at[:, d]))
        out_copies.append(begin(ov.at[pl.ds(0, nx), d], mine_hbm.at[:, d]))
    ct_in.wait()
    for d in range(nz):
        res = jnp.dot(ctv[d], hidden, preferred_element_type=F32)
        res = (0.5 * res).astype(BF16)
        high = sums[d].astype(BF16)
        left = sums[d] - high.astype(F32)
        mid = left.astype(BF16)
        low = (left - mid.astype(F32)).astype(BF16)
        extra = jnp.concatenate([high, mid, low, jnp.zeros((5, cols), BF16)], axis=0)
        extra = jnp.concatenate([extra, jnp.zeros((8, units - cols), BF16)], axis=1)
        for y in range(ny):
            dv[y, d, :rows] = res[y * rows : (y + 1) * rows]
            dv[y, d, rows:] = extra
        out_copies.append(begin(dv.at[:, d], dd_hbm.at[:, d]))
    for copy in out_copies:
        copy.wait()


def rows_kernel(at_ref, got_ref, out_ref):
    ny, nz, longer, _ = got_ref.shape
    rows = longer - 8
    half = rows // 2
    sums = []
    for d in range(nz):
        total = got_ref[0, d].astype(F32)
        for k in range(1, ny):
            total = total + got_ref[k, d].astype(F32)
        part = total[:rows].astype(BF16)
        to = (at_ref[0] + d) % nz
        out_ref[to, :half] = part[:half]
        out_ref[nz + to, :half] = part[half:]
        sums.append(jnp.sum(total[rows:], axis=0, keepdims=True))
    extra = jnp.concatenate(sums, axis=0)
    extra = pltpu.roll(extra, at_ref[0], 0).astype(BF16)
    for k in range(2 * nz):
        out_ref[k, half:] = extra


def ring_kernel(got_ref, out_ref, sum_ref):
    half = out_ref.shape[0]
    cols = sum_ref.shape[2]
    total = got_ref[0].astype(F32)
    for k in range(1, got_ref.shape[0]):
        total = total + got_ref[k].astype(F32)
    out_ref[...] = total[:half]
    for k in range(sum_ref.shape[0]):
        sum_ref[k] = total[half:, :cols]


def chip_kernel(mine_ref, theirs_ref, *out_refs):
    for k, out_ref in enumerate(out_refs):
        out_ref[...] = (mine_ref[k].astype(F32) + theirs_ref[k].astype(F32)).astype(BF16)


def finish_kernel(at_ref, got0, got1, got2, got3, x_ref, c_ref, gain_ref, out_ref, dn_ref):
    nz, _, cols = got0.shape
    for d in range(nz):
        own = pl.ds(pl.multiple_of(((at_ref[0] + d) % nz) * cols, cols), cols)
        total = got0[d].astype(F32)
        for got in (got1, got2, got3):
            total = total + got[d].astype(F32)
        dn_ref[:, own] = total.astype(BF16)
    v = x_ref[...].astype(F32)
    inv = lax.rsqrt(jnp.mean(v * v, axis=-1, keepdims=True) + EPS)
    xhat = v * inv
    dn = dn_ref[...].astype(F32)
    gs = gain_ref[...] * dn
    m = jnp.mean(gs * xhat, axis=-1, keepdims=True)
    out_ref[...] = (c_ref[...].astype(F32) + inv * (gs - xhat * m)).astype(BF16)


def place_kernel(at_ref, p0, p1, p2, p3, other_ref, out_ref):
    n = 4
    part = out_ref.shape[0] // (2 * n)
    for k, piece in enumerate((p0, p1, p2, p3)):
        spot = (at_ref[2] + k) % n
        own = pl.multiple_of((at_ref[1] * n + spot) * part, part)
        far = pl.multiple_of(((1 - at_ref[1]) * n + spot) * part, part)
        out_ref[pl.ds(own, part), :] = piece[:part]
        out_ref[pl.ds(far, part), :] = other_ref[k, :part]


def near(*arrays):
    return [pltpu.with_memory_space_constraint(a, pltpu.VMEM) for a in arrays]


def vmem(n):
    return [pl.BlockSpec(memory_space=pltpu.VMEM)] * n


def work(inputs, gain, gate_weight, up_weight, down_weight, cotangent):
    nz, ny, nx = lax.axis_size("fs_0"), lax.axis_size("fs_1"), lax.axis_size("x")
    rep, zl = lax.axis_index("rep"), lax.axis_index("fs_0")
    x, c = lax.axis_index("x"), lax.axis_index("c")
    tokens, width = inputs.shape
    rows, units = gate_weight.shape
    cols = width // nz
    part = tokens // 2 // nx
    gain2 = gain[None]
    at = jnp.stack([zl, c, x]).astype(jnp.int32)

    w = jnp.concatenate([gate_weight, up_weight, down_weight], axis=1)
    w0 = from_all(w, "fs_1").reshape(ny * rows, 3 * units)
    fwd, bwd = [w0], [w0]
    for _ in range(3):
        fwd.append(shifted(fwd[-1], RING, 1))
        bwd.append(shifted(bwd[-1], RING, -1))
    mid = cols // 2
    last_f = shifted(fwd[-1][:mid], RING, 1)
    last_b = shifted(bwd[-1][mid:], RING, -1)
    weights = [w0, bwd[1], bwd[2], bwd[3], fwd[3], fwd[2], fwd[1]]

    def spot(i, at):
        return ((i // nx + at[1]) % 2) * nx + (i + at[2]) % nx

    xr = pl.pallas_call(
        prepare_tokens,
        out_shape=jax.ShapeDtypeStruct((nz, tokens, cols), BF16),
        grid_spec=pltpu.PrefetchScalarGridSpec(
            num_scalar_prefetch=1,
            grid=(2 * nx,),
            in_specs=[
                pl.BlockSpec((part, width), lambda i, at: (spot(i, at), 0)),
                pl.BlockSpec((1, width), lambda i, at: (0, 0)),
            ],
            out_specs=pl.BlockSpec((nz, part, cols), lambda i, at: (0, i, 0)),
        ),
        name="prepare_x",
    )(at, inputs, gain2)
    cr, ct = pl.pallas_call(
        prepare_cotangent,
        out_shape=(
            jax.ShapeDtypeStruct((nz, tokens, cols), BF16),
            jax.ShapeDtypeStruct((nz, cols, tokens), BF16),
        ),
        grid_spec=pltpu.PrefetchScalarGridSpec(
            num_scalar_prefetch=1,
            grid=(nx,),
            in_specs=[
                pl.BlockSpec((part, width), lambda i, at: (spot(2 * i, at), 0)),
                pl.BlockSpec((part, width), lambda i, at: (spot(2 * i + 1, at), 0)),
            ],
            out_specs=(
                pl.BlockSpec((nz, 2 * part, cols), lambda i, at: (0, i, 0)),
                pl.BlockSpec((nz, cols, 2 * part), lambda i, at: (0, 0, i)),
            ),
        ),
        name="prepare_c",
    )(at, cotangent, cotangent)

    gain_ring = rolled(gain.reshape(nz, 1, cols), zl)
    acc = pl.pallas_call(
        forward_kernel,
        out_shape=jax.ShapeDtypeStruct((tokens, 3 * units), F32),
        in_specs=vmem(7),
        out_specs=pl.BlockSpec(memory_space=pltpu.VMEM),
        name="forward",
    )(xr, cr, w0, bwd[1], fwd[1], bwd[2], fwd[2])
    anywhere = pl.BlockSpec(memory_space=pl.ANY)
    mine, other, dd = pl.pallas_call(
        grad_kernel,
        out_shape=(
            jax.ShapeDtypeStruct((nx, nz, part, cols), BF16),
            jax.ShapeDtypeStruct((nx, nz, part, cols), BF16),
            jax.ShapeDtypeStruct((ny, nz, rows + 8, units), BF16),
        ),
        in_specs=vmem(3) + [anywhere] * 11,
        out_specs=(anywhere,) * 3,
        scratch_shapes=[
            pltpu.VMEM((tokens, 3 * units), F32),
            pltpu.VMEM((nz, tokens, cols), BF16),
            pltpu.VMEM((3, tokens, cols), BF16),
            pltpu.VMEM((nz, cols, tokens), BF16),
            pltpu.VMEM((7, cols, 3 * units), BF16),
            pltpu.VMEM((2 * nx, nz, part, cols), BF16),
            pltpu.VMEM((ny, nz, rows + 8, units), BF16),
            pltpu.SemaphoreType.DMA((48,)),
        ],
        name="grad",
    )(gain_ring, *near(last_f, last_b), acc, xr, cr, ct, *weights)
    theirs = shifted(other, "c", 1)
    dy = exchanged(dd, "fs_1")

    chunk = jax.ShapeDtypeStruct((nz, part, cols), BF16)
    chip = pl.pallas_call(
        chip_kernel,
        out_shape=(chunk,) * 4,
        in_specs=vmem(2),
        out_specs=tuple(vmem(4)),
        name="chip",
    )(mine, *near(theirs))
    got = [chip[0]]
    for k in (1, 2, 3):
        got.append(shifted(chip[k], "x", k))
    own = pl.BlockSpec((part, width), lambda i, at: (at[1] * nx + at[2], 0))
    ig = pl.pallas_call(
        finish_kernel,
        out_shape=jax.ShapeDtypeStruct((part, width), BF16),
        grid_spec=pltpu.PrefetchScalarGridSpec(
            num_scalar_prefetch=1,
            grid=(1,),
            in_specs=vmem(4) + [own, own, pl.BlockSpec((1, width), lambda i, at: (0, 0))],
            out_specs=pl.BlockSpec((part, width), lambda i, at: (0, 0)),
            scratch_shapes=[pltpu.VMEM((part, width), BF16)],
        ),
        name="finish",
    )(at, got[0], *near(*got[1:]), inputs, cotangent, gain2)
    pieces = [ig]
    for k in (1, 2, 3):
        pieces.append(shifted(ig, "x", -k))
    ig_other = shifted(jnp.stack(pieces), "c", 1)
    out = pl.pallas_call(
        place_kernel,
        out_shape=jax.ShapeDtypeStruct((tokens, width), BF16),
        in_specs=[pl.BlockSpec(memory_space=pltpu.SMEM)] + vmem(5),
        out_specs=pl.BlockSpec(memory_space=pltpu.VMEM),
        name="place",
    )(at, pieces[0], *near(*pieces[1:], ig_other))

    dz = pl.pallas_call(
        rows_kernel,
        out_shape=jax.ShapeDtypeStruct((2 * nz, rows // 2 + 8, units), BF16),
        in_specs=[pl.BlockSpec(memory_space=pltpu.SMEM)] + vmem(1),
        out_specs=pl.BlockSpec(memory_space=pltpu.VMEM),
        name="ysum",
    )(at, *near(dy))
    dz = exchanged(dz, RING)
    own, gain_own = pl.pallas_call(
        ring_kernel,
        out_shape=(
            jax.ShapeDtypeStruct((rows // 2, units), F32),
            jax.ShapeDtypeStruct((lax.axis_size(TP), nz, cols), F32),
        ),
        in_specs=vmem(1),
        out_specs=tuple(vmem(2)),
        name="zsum",
    )(*near(dz))
    gain_all = exchanged(gain_own, TP)
    gain_gradient = jnp.sum(gain_all, axis=0).reshape(width)
    far = shifted(own, "rep", 1)
    pair = rolled(jnp.stack([own, far]), rep)
    d_down = pair.reshape(rows, units)
    return (out, gain_gradient, d_down)


def solution(mesh):
    torus = Mesh(
        mesh.devices.reshape(mesh.shape["rep"], 8, 4, 4, 2),
        ("rep", "fs_0", "fs_1", "x", "c"),
    )
    return jax.shard_map(
        work,
        mesh=torus,
        in_specs=(P(REP_FS, None), P(), P(FS, TP), P(FS, TP), P(FS, TP), P(REP_FS, None)),
        out_specs=(P(REP_FS, None), P(), P(FS, TP)),
        check_vma=False,
    )
```

```python
import jax
import jax.numpy as jnp
from jax import lax
from jax.experimental import pallas as pl
from jax.experimental.pallas import tpu as pltpu
from jax.sharding import Mesh
from jax.sharding import PartitionSpec as P

FS = ("fs_0", "fs_1")
REP_FS = ("rep", "fs_0", "fs_1")
TP = ("x", "c")
RING = ("rep", "fs_0")
EPS = 1e-06
LANES = 128
TILES = 3
EARLY = (0, 1, 7, 2, 6)
F32 = jnp.float32
BF16 = jnp.bfloat16


def shifted(v, axis, by):
    n = lax.axis_size(axis)
    return lax.ppermute(v, axis, [(i, (i + by) % n) for i in range(n)])


def exchanged(v, axis):
    return lax.all_to_all(v, axis, 0, 0, tiled=True)


def from_all(v, axis):
    n = lax.axis_size(axis)
    return exchanged(jnp.broadcast_to(v[None], (n, *v.shape)), axis)


def rolled(v, start):
    return lax.dynamic_slice_in_dim(jnp.concatenate([v, v], axis=0), start, v.shape[0], axis=0)


def prepare_tokens(at_ref, x_ref, gain_ref, out_ref):
    nz, _, cols = out_ref.shape
    v = x_ref[...].astype(F32)
    inv = lax.rsqrt(jnp.mean(v * v, axis=-1, keepdims=True) + EPS)
    for d in range(nz):
        own = pl.ds(pl.multiple_of(((at_ref[0] + d) % nz) * cols, cols), cols)
        part = x_ref[:, own].astype(F32)
        out_ref[d] = (part * inv * gain_ref[:, own]).astype(BF16)


def prepare_cotangent(at_ref, lo_ref, hi_ref, out_ref, turned_ref):
    nz, _, cols = out_ref.shape
    for d in range(nz):
        own = pl.ds(pl.multiple_of(((at_ref[0] + d) % nz) * cols, cols), cols)
        part = jnp.concatenate([lo_ref[:, own], hi_ref[:, own]], axis=0)
        out_ref[d] = part
        turned_ref[d] = part.T


def forward_kernel(x_ref, c_ref, *refs):
    w_refs, acc_ref = refs[:-1], refs[-1]
    units = acc_ref.shape[1] // 3
    gu = dh = None
    for d, w in zip(EARLY, w_refs):
        a = jnp.dot(x_ref[d], w[:, : 2 * units], preferred_element_type=F32)
        b = jnp.dot(c_ref[d], w[:, 2 * units :], preferred_element_type=F32)
        gu = a if gu is None else gu + a
        dh = b if dh is None else dh + b
    acc_ref[:, : 2 * units] = gu
    acc_ref[:, 2 * units :] = dh


def grad_kernel(gain_ref, lo_ref, hi_ref, acc_hbm, x_hbm, c_hbm, ct_hbm, *refs):
    w_hbm, (mine_hbm, other_hbm, dd_hbm) = refs[:7], refs[7:10]
    acc, xv, cv, ctv, wv, ov, dv, sems = refs[10:]
    units = acc.shape[1] // 3
    nz, _, cols = xv.shape
    ny, _, longer, _ = dv.shape
    nx, part = mine_hbm.shape[0], mine_hbm.shape[2]
    tiles = units // LANES
    rows = (longer - 8) // tiles
    used = [0]

    def begin(src, dst):
        copy = pltpu.make_async_copy(src, dst, sems.at[used[0]])
        used[0] += 1
        copy.start()
        return copy

    slot = {0: 0, 1: 1, 2: 2, 3: 3, 5: 4, 6: 5, 7: 6}
    acc_in = begin(acc_hbm, acc)
    x_in, c_in, w_in = {}, {}, {}
    for d in (3, 5):
        w_in[d] = begin(w_hbm[slot[d]], wv.at[slot[d]])
        x_in[d] = begin(x_hbm.at[d], xv.at[d])
        c_in[d] = begin(c_hbm.at[d], cv.at[d - 3])
    x_in[4] = begin(x_hbm.at[4], xv.at[4])
    c_in[4] = begin(c_hbm.at[4], cv.at[1])

    half = cols // 2
    halves = ((lo_ref, slice(0, half)), (hi_ref, slice(half, cols)))
    acc_in.wait()
    gu, dh = acc[:, : 2 * units], acc[:, 2 * units :]
    for d in (3, 5):
        w_in[d].wait()
        x_in[d].wait()
        c_in[d].wait()
        for e in EARLY if d == 3 else ():
            w_in[e] = begin(w_hbm[slot[e]], wv.at[slot[e]])
            x_in[e] = begin(x_hbm.at[e], xv.at[e])
        w = wv.at[slot[d]]
        gu = gu + jnp.dot(xv[d], w[:, : 2 * units], preferred_element_type=F32)
        dh = dh + jnp.dot(cv[d - 3], w[:, 2 * units :], preferred_element_type=F32)
    x_in[4].wait()
    c_in[4].wait()
    for w, at in halves:
        gu = gu + jnp.dot(xv[4, :, at], w[:, : 2 * units], preferred_element_type=F32)
        dh = dh + jnp.dot(cv[1, :, at], w[:, 2 * units :], preferred_element_type=F32)
    gate, up = gu[:, :units], gu[:, units:]
    dh = 0.5 * dh
    sig = jax.nn.sigmoid(gate)
    act = gate * sig
    hidden = (act * up).astype(BF16)
    d_gate = (dh * up * sig * (1.0 + gate * (1.0 - sig))).astype(BF16)
    d_up = (dh * act).astype(BF16)
    both = jnp.concatenate([d_gate, d_up], axis=1)
    ct_in = begin(ct_hbm, ctv)
    out_copies = []
    sums = {}
    for d in (4, 3, 5) + EARLY:
        if d in EARLY:
            w_in[d].wait()
            x_in[d].wait()
        pieces = halves if d == 4 else ((wv.at[slot[d]], slice(0, cols)),)
        got = []
        for w, at in pieces:
            out = lax.dot_general(
                both, w[:, : 2 * units], (((1,), (1,)), ((), ())), preferred_element_type=F32
            )
            terms = jnp.sum(xv[d, :, at].astype(F32) * out, axis=0, keepdims=True)
            got.append(terms / gain_ref[d, :, at])
            out = out.astype(BF16)
            for k in range(2 * nx):
                ov[k, d, :, at] = out[k * part : (k + 1) * part]
        sums[d] = got[0] if len(got) == 1 else jnp.concatenate(got, axis=1)
        out_copies.append(begin(ov.at[pl.ds(nx, nx), d], other_hbm.at[:, d]))
        out_copies.append(begin(ov.at[pl.ds(0, nx), d], mine_hbm.at[:, d]))
    ct_in.wait()
    for d in range(nz):
        res = jnp.dot(ctv[d], hidden, preferred_element_type=F32)
        res = (0.5 * res).astype(BF16)
        high = sums[d].astype(BF16)
        left = sums[d] - high.astype(F32)
        mid = left.astype(BF16)
        low = (left - mid.astype(F32)).astype(BF16)
        ends = [v[:, at : at + LANES] for at in (0, LANES) for v in (high, mid, low)]
        extra = jnp.concatenate(ends + [jnp.zeros((2, LANES), BF16)], axis=0)
        for y in range(ny):
            for j in range(tiles):
                dv[y, d, j * rows : (j + 1) * rows] = res[
                    y * rows : (y + 1) * rows, j * LANES : (j + 1) * LANES
                ]
            dv[y, d, tiles * rows :] = extra
        out_copies.append(begin(dv.at[:, d], dd_hbm.at[:, d]))
    for copy in out_copies:
        copy.wait()


def rows_kernel(at_ref, got_ref, out_ref):
    ny, nz, longer, _ = got_ref.shape
    ends = out_ref.shape[1] - 16
    rows = (longer - 8) // TILES
    tiles = TILES
    half = rows // 2
    sums = []
    for d in range(nz):
        total = got_ref[0, d].astype(F32)
        for k in range(1, ny):
            total = total + got_ref[k, d].astype(F32)
        to = (at_ref[0] + d) % nz
        for j in range(tiles):
            part = total[j * rows : (j + 1) * rows].astype(BF16)
            out_ref[to, j * half : (j + 1) * half] = part[:half]
            out_ref[nz + to, j * half : (j + 1) * half] = part[half:]
        base = tiles * rows
        one = jnp.sum(total[base : base + 3], axis=0, keepdims=True)
        two = jnp.sum(total[base + 3 : base + 6], axis=0, keepdims=True)
        sums.append(jnp.concatenate([one, two], axis=1))
    extra = jnp.concatenate(sums, axis=0)
    extra = pltpu.roll(extra, at_ref[0], 0).astype(BF16)
    for k in range(2 * nz):
        out_ref[k, ends : ends + 8] = extra[:, :LANES]
        out_ref[k, ends + 8 :] = extra[:, LANES:]


def ring_kernel(got_ref, out_ref, short_ref, sum_ref):
    half, units = out_ref.shape
    tiles = units // LANES
    total = got_ref[0].astype(F32)
    for k in range(1, got_ref.shape[0]):
        total = total + got_ref[k].astype(F32)
    for j in range(tiles):
        part = total[j * half : (j + 1) * half]
        out_ref[:, j * LANES : (j + 1) * LANES] = part
        short_ref[:, j * LANES : (j + 1) * LANES] = part.astype(BF16)
    ends = tiles * half
    for k in range(sum_ref.shape[0]):
        sum_ref[k, :, :LANES] = total[ends : ends + 8]
        sum_ref[k, :, LANES:] = total[ends + 8 :]


def chip_kernel(mine_ref, theirs_ref, *out_refs):
    for k, out_ref in enumerate(out_refs):
        out_ref[...] = (mine_ref[k].astype(F32) + theirs_ref[k].astype(F32)).astype(BF16)


def finish_kernel(at_ref, got0, got1, got2, got3, x_ref, c_ref, gain_ref, out_ref, dn_ref):
    nz, _, cols = got0.shape
    for d in range(nz):
        own = pl.ds(pl.multiple_of(((at_ref[0] + d) % nz) * cols, cols), cols)
        total = got0[d].astype(F32)
        for got in (got1, got2, got3):
            total = total + got[d].astype(F32)
        dn_ref[:, own] = total.astype(BF16)
    v = x_ref[...].astype(F32)
    inv = lax.rsqrt(jnp.mean(v * v, axis=-1, keepdims=True) + EPS)
    xhat = v * inv
    dn = dn_ref[...].astype(F32)
    gs = gain_ref[...] * dn
    m = jnp.mean(gs * xhat, axis=-1, keepdims=True)
    out_ref[...] = (c_ref[...].astype(F32) + inv * (gs - xhat * m)).astype(BF16)


def place_kernel(at_ref, p0, p1, p2, p3, other_ref, out_ref):
    n = 4
    part = out_ref.shape[0] // (2 * n)
    for k, piece in enumerate((p0, p1, p2, p3)):
        spot = (at_ref[2] + k) % n
        own = pl.multiple_of((at_ref[1] * n + spot) * part, part)
        far = pl.multiple_of(((1 - at_ref[1]) * n + spot) * part, part)
        out_ref[pl.ds(own, part), :] = piece[:part]
        out_ref[pl.ds(far, part), :] = other_ref[k, :part]


def near(*arrays):
    return [pltpu.with_memory_space_constraint(a, pltpu.VMEM) for a in arrays]


def vmem(n):
    return [pl.BlockSpec(memory_space=pltpu.VMEM)] * n


def work(inputs, gain, gate_weight, up_weight, down_weight, cotangent):
    nz, ny, nx = lax.axis_size("fs_0"), lax.axis_size("fs_1"), lax.axis_size("x")
    rep, zl = lax.axis_index("rep"), lax.axis_index("fs_0")
    x, c = lax.axis_index("x"), lax.axis_index("c")
    tokens, width = inputs.shape
    rows, units = gate_weight.shape
    cols = width // nz
    part = tokens // 2 // nx
    gain2 = gain[None]
    at = jnp.stack([zl, c, x]).astype(jnp.int32)

    w = jnp.concatenate([gate_weight, up_weight, down_weight], axis=1)
    w0 = from_all(w, "fs_1").reshape(ny * rows, 3 * units)
    fwd, bwd = [w0], [w0]
    for _ in range(3):
        fwd.append(shifted(fwd[-1], RING, 1))
        bwd.append(shifted(bwd[-1], RING, -1))
    mid = cols // 2
    last_f = shifted(fwd[-1][:mid], RING, 1)
    last_b = shifted(bwd[-1][mid:], RING, -1)
    weights = [w0, bwd[1], bwd[2], bwd[3], fwd[3], fwd[2], fwd[1]]

    def spot(i, at):
        return ((i // nx + at[1]) % 2) * nx + (i + at[2]) % nx

    xr = pl.pallas_call(
        prepare_tokens,
        out_shape=jax.ShapeDtypeStruct((nz, tokens, cols), BF16),
        grid_spec=pltpu.PrefetchScalarGridSpec(
            num_scalar_prefetch=1,
            grid=(2 * nx,),
            in_specs=[
                pl.BlockSpec((part, width), lambda i, at: (spot(i, at), 0)),
                pl.BlockSpec((1, width), lambda i, at: (0, 0)),
            ],
            out_specs=pl.BlockSpec((nz, part, cols), lambda i, at: (0, i, 0)),
        ),
        name="prepare_x",
    )(at, inputs, gain2)
    cr, ct = pl.pallas_call(
        prepare_cotangent,
        out_shape=(
            jax.ShapeDtypeStruct((nz, tokens, cols), BF16),
            jax.ShapeDtypeStruct((nz, cols, tokens), BF16),
        ),
        grid_spec=pltpu.PrefetchScalarGridSpec(
            num_scalar_prefetch=1,
            grid=(nx,),
            in_specs=[
                pl.BlockSpec((part, width), lambda i, at: (spot(2 * i, at), 0)),
                pl.BlockSpec((part, width), lambda i, at: (spot(2 * i + 1, at), 0)),
            ],
            out_specs=(
                pl.BlockSpec((nz, 2 * part, cols), lambda i, at: (0, i, 0)),
                pl.BlockSpec((nz, cols, 2 * part), lambda i, at: (0, 0, i)),
            ),
        ),
        name="prepare_c",
    )(at, cotangent, cotangent)

    gain_ring = rolled(gain.reshape(nz, 1, cols), zl)
    acc = pl.pallas_call(
        forward_kernel,
        out_shape=jax.ShapeDtypeStruct((tokens, 3 * units), F32),
        in_specs=vmem(7),
        out_specs=pl.BlockSpec(memory_space=pltpu.VMEM),
        name="forward",
    )(xr, cr, w0, bwd[1], fwd[1], bwd[2], fwd[2])
    anywhere = pl.BlockSpec(memory_space=pl.ANY)
    mine, other, dd = pl.pallas_call(
        grad_kernel,
        out_shape=(
            jax.ShapeDtypeStruct((nx, nz, part, cols), BF16),
            jax.ShapeDtypeStruct((nx, nz, part, cols), BF16),
            jax.ShapeDtypeStruct((ny, nz, TILES * rows + 8, LANES), BF16),
        ),
        in_specs=vmem(3) + [anywhere] * 11,
        out_specs=(anywhere,) * 3,
        scratch_shapes=[
            pltpu.VMEM((tokens, 3 * units), F32),
            pltpu.VMEM((nz, tokens, cols), BF16),
            pltpu.VMEM((3, tokens, cols), BF16),
            pltpu.VMEM((nz, cols, tokens), BF16),
            pltpu.VMEM((7, cols, 3 * units), BF16),
            pltpu.VMEM((2 * nx, nz, part, cols), BF16),
            pltpu.VMEM((ny, nz, TILES * rows + 8, LANES), BF16),
            pltpu.SemaphoreType.DMA((48,)),
        ],
        name="grad",
    )(gain_ring, *near(last_f, last_b), acc, xr, cr, ct, *weights)
    theirs = shifted(other, "c", 1)
    dy = exchanged(dd, "fs_1")

    chunk = jax.ShapeDtypeStruct((nz, part, cols), BF16)
    chip = pl.pallas_call(
        chip_kernel,
        out_shape=(chunk,) * 4,
        in_specs=vmem(2),
        out_specs=tuple(vmem(4)),
        name="chip",
    )(mine, *near(theirs))
    got = [chip[0]]
    for k in (1, 2, 3):
        got.append(shifted(chip[k], "x", k))
    own = pl.BlockSpec((part, width), lambda i, at: (at[1] * nx + at[2], 0))
    ig = pl.pallas_call(
        finish_kernel,
        out_shape=jax.ShapeDtypeStruct((part, width), BF16),
        grid_spec=pltpu.PrefetchScalarGridSpec(
            num_scalar_prefetch=1,
            grid=(1,),
            in_specs=vmem(4) + [own, own, pl.BlockSpec((1, width), lambda i, at: (0, 0))],
            out_specs=pl.BlockSpec((part, width), lambda i, at: (0, 0)),
            scratch_shapes=[pltpu.VMEM((part, width), BF16)],
        ),
        name="finish",
    )(at, got[0], *near(*got[1:]), inputs, cotangent, gain2)
    pieces = [ig]
    for k in (1, 2, 3):
        pieces.append(shifted(ig, "x", -k))
    ig_other = shifted(jnp.stack(pieces), "c", 1)
    out = pl.pallas_call(
        place_kernel,
        out_shape=jax.ShapeDtypeStruct((tokens, width), BF16),
        in_specs=[pl.BlockSpec(memory_space=pltpu.SMEM)] + vmem(5),
        out_specs=pl.BlockSpec(memory_space=pltpu.VMEM),
        name="place",
    )(at, pieces[0], *near(*pieces[1:], ig_other))

    dz = pl.pallas_call(
        rows_kernel,
        out_shape=jax.ShapeDtypeStruct((2 * nz, TILES * rows // 2 + 16, LANES), BF16),
        in_specs=[pl.BlockSpec(memory_space=pltpu.SMEM)] + vmem(1),
        out_specs=pl.BlockSpec(memory_space=pltpu.VMEM),
        name="ysum",
    )(at, *near(dy))
    dz = exchanged(dz, RING)
    own, short, gain_own = pl.pallas_call(
        ring_kernel,
        out_shape=(
            jax.ShapeDtypeStruct((rows // 2, units), F32),
            jax.ShapeDtypeStruct((rows // 2, units), BF16),
            jax.ShapeDtypeStruct((lax.axis_size(TP), nz, cols), F32),
        ),
        in_specs=vmem(1),
        out_specs=tuple(vmem(3)),
        name="zsum",
    )(*near(dz))
    gain_all = exchanged(gain_own, TP)
    gain_gradient = jnp.sum(gain_all, axis=0).reshape(width)
    far = shifted(short, "rep", 1).astype(F32)
    pair = rolled(jnp.stack([own, far]), rep)
    d_down = pair.reshape(rows, units)
    return (out, gain_gradient, d_down)


def solution(mesh):
    torus = Mesh(
        mesh.devices.reshape(mesh.shape["rep"], 8, 4, 4, 2),
        ("rep", "fs_0", "fs_1", "x", "c"),
    )
    return jax.shard_map(
        work,
        mesh=torus,
        in_specs=(P(REP_FS, None), P(), P(FS, TP), P(FS, TP), P(FS, TP), P(REP_FS, None)),
        out_specs=(P(REP_FS, None), P(), P(FS, TP)),
        check_vma=False,
    )
```

```python
import jax
import jax.numpy as jnp
from jax import lax
from jax.experimental import pallas as pl
from jax.experimental.pallas import tpu as pltpu
from jax.sharding import Mesh
from jax.sharding import PartitionSpec as P

FS = ("fs_0", "fs_1")
REP_FS = ("rep", "fs_0", "fs_1")
TP = ("x", "c")
RING = ("rep", "fs_0")
EPS = 1e-06
LANES = 128
TILES = 3
EARLY = (0, 1, 7, 2, 6)
F32 = jnp.float32
BF16 = jnp.bfloat16


def shifted(v, axis, by):
    n = lax.axis_size(axis)
    return lax.ppermute(v, axis, [(i, (i + by) % n) for i in range(n)])


def exchanged(v, axis):
    return lax.all_to_all(v, axis, 0, 0, tiled=True)


def from_all(v, axis):
    n = lax.axis_size(axis)
    return exchanged(jnp.broadcast_to(v[None], (n, *v.shape)), axis)


def rolled(v, start):
    return lax.dynamic_slice_in_dim(jnp.concatenate([v, v], axis=0), start, v.shape[0], axis=0)


def prepare_tokens(at_ref, x_ref, gain_ref, out_ref, own_ref):
    @pl.when(pl.program_id(0) == 0)
    def _():
        own_ref[...] = x_ref[...]

    nz, _, cols = out_ref.shape
    v = x_ref[...].astype(F32)
    inv = lax.rsqrt(jnp.mean(v * v, axis=-1, keepdims=True) + EPS)
    for d in range(nz):
        own = pl.ds(pl.multiple_of(((at_ref[0] + d) % nz) * cols, cols), cols)
        part = x_ref[:, own].astype(F32)
        out_ref[d] = (part * inv * gain_ref[:, own]).astype(BF16)


def prepare_cotangent(at_ref, lo_ref, hi_ref, out_ref, turned_ref, own_ref):
    @pl.when(pl.program_id(0) == 0)
    def _():
        own_ref[...] = lo_ref[...]

    nz, _, cols = out_ref.shape
    for d in range(nz):
        own = pl.ds(pl.multiple_of(((at_ref[0] + d) % nz) * cols, cols), cols)
        part = jnp.concatenate([lo_ref[:, own], hi_ref[:, own]], axis=0)
        out_ref[d] = part
        turned_ref[d] = part.T


def forward_kernel(x_ref, c_ref, *refs):
    w_refs, acc_ref = refs[:-1], refs[-1]
    units = acc_ref.shape[1] // 3
    gu = dh = None
    for d, w in zip(EARLY, w_refs):
        a = jnp.dot(x_ref[d], w[:, : 2 * units], preferred_element_type=F32)
        b = jnp.dot(c_ref[d], w[:, 2 * units :], preferred_element_type=F32)
        gu = a if gu is None else gu + a
        dh = b if dh is None else dh + b
    acc_ref[:, : 2 * units] = gu
    acc_ref[:, 2 * units :] = dh


def grad_kernel(gain_ref, lo_ref, hi_ref, acc_hbm, x_hbm, c_hbm, ct_hbm, *refs):
    w_hbm, (mine_hbm, other_hbm, dd_hbm) = refs[:7], refs[7:10]
    acc, xv, cv, ctv, wv, ev, ov, dv, sems = refs[10:]
    units = acc.shape[1] // 3
    nz, _, cols = xv.shape
    ny, _, longer, _ = dv.shape
    nx, part = mine_hbm.shape[0], mine_hbm.shape[2]
    tiles = units // LANES
    rows = (longer - 8) // tiles
    used = [0]

    def begin(src, dst):
        copy = pltpu.make_async_copy(src, dst, sems.at[used[0]])
        used[0] += 1
        copy.start()
        return copy

    slot = {0: 0, 1: 1, 2: 2, 3: 3, 5: 4, 6: 5, 7: 6}
    acc_in = begin(acc_hbm, acc)
    x_in, c_in, w_in = {}, {}, {}
    for d in (3, 5):
        w_in[d] = begin(w_hbm[slot[d]], wv.at[(d - 3) // 2])
        x_in[d] = begin(x_hbm.at[d], xv.at[d])
        c_in[d] = begin(c_hbm.at[d], cv.at[d - 3])
    x_in[4] = begin(x_hbm.at[4], xv.at[4])
    c_in[4] = begin(c_hbm.at[4], cv.at[1])

    half = cols // 2
    halves = ((lo_ref, slice(0, half)), (hi_ref, slice(half, cols)))
    acc_in.wait()
    gu, dh = acc[:, : 2 * units], acc[:, 2 * units :]
    for d in (3, 5):
        w_in[d].wait()
        x_in[d].wait()
        c_in[d].wait()
        for i, e in enumerate(EARLY) if d == 3 else ():
            w_in[e] = begin(w_hbm[slot[e]].at[:, pl.ds(0, 2 * units)], ev.at[i])
            x_in[e] = begin(x_hbm.at[e], xv.at[e])
        w = wv.at[(d - 3) // 2]
        gu = gu + jnp.dot(xv[d], w[:, : 2 * units], preferred_element_type=F32)
        dh = dh + jnp.dot(cv[d - 3], w[:, 2 * units :], preferred_element_type=F32)
    x_in[4].wait()
    c_in[4].wait()
    for w, at in halves:
        gu = gu + jnp.dot(xv[4, :, at], w[:, : 2 * units], preferred_element_type=F32)
        dh = dh + jnp.dot(cv[1, :, at], w[:, 2 * units :], preferred_element_type=F32)
    gate, up = gu[:, :units], gu[:, units:]
    dh = 0.5 * dh
    sig = jax.nn.sigmoid(gate)
    act = gate * sig
    hidden = (act * up).astype(BF16)
    d_gate = (dh * up * sig * (1.0 + gate * (1.0 - sig))).astype(BF16)
    d_up = (dh * act).astype(BF16)
    both = jnp.concatenate([d_gate, d_up], axis=1)
    ct_in = begin(ct_hbm, ctv)
    out_copies = []
    sums = {}
    for d in (4, 3, 5) + EARLY:
        if d in EARLY:
            w_in[d].wait()
            x_in[d].wait()
        if d == 4:
            pieces = halves
        else:
            block = ev.at[EARLY.index(d)] if d in EARLY else wv.at[(d - 3) // 2]
            pieces = ((block, slice(0, cols)),)
        got = []
        for w, at in pieces:
            out = lax.dot_general(
                both, w[:, : 2 * units], (((1,), (1,)), ((), ())), preferred_element_type=F32
            )
            terms = jnp.sum(xv[d, :, at].astype(F32) * out, axis=0, keepdims=True)
            got.append(terms / gain_ref[d, :, at])
            out = out.astype(BF16)
            for k in range(2 * nx):
                ov[k, d, :, at] = out[k * part : (k + 1) * part]
        sums[d] = got[0] if len(got) == 1 else jnp.concatenate(got, axis=1)
        out_copies.append(begin(ov.at[pl.ds(nx, nx), d], other_hbm.at[:, d]))
        out_copies.append(begin(ov.at[pl.ds(0, nx), d], mine_hbm.at[:, d]))
    ct_in.wait()
    for d in range(nz):
        res = jnp.dot(ctv[d], hidden, preferred_element_type=F32)
        res = (0.5 * res).astype(BF16)
        high = sums[d].astype(BF16)
        left = sums[d] - high.astype(F32)
        mid = left.astype(BF16)
        low = (left - mid.astype(F32)).astype(BF16)
        ends = [v[:, at : at + LANES] for at in (0, LANES) for v in (high, mid, low)]
        extra = jnp.concatenate(ends + [jnp.zeros((2, LANES), BF16)], axis=0)
        for y in range(ny):
            for j in range(tiles):
                dv[y, d, j * rows : (j + 1) * rows] = res[
                    y * rows : (y + 1) * rows, j * LANES : (j + 1) * LANES
                ]
            dv[y, d, tiles * rows :] = extra
        out_copies.append(begin(dv.at[:, d], dd_hbm.at[:, d]))
    for copy in out_copies:
        copy.wait()


def rows_kernel(at_ref, got_ref, out_ref):
    ny, nz, longer, _ = got_ref.shape
    ends = out_ref.shape[1] - 16
    rows = (longer - 8) // TILES
    tiles = TILES
    half = rows // 2
    sums = []
    for d in range(nz):
        total = got_ref[0, d].astype(F32)
        for k in range(1, ny):
            total = total + got_ref[k, d].astype(F32)
        to = (at_ref[0] + d) % nz
        for j in range(tiles):
            part = total[j * rows : (j + 1) * rows].astype(BF16)
            out_ref[to, j * half : (j + 1) * half] = part[:half]
            out_ref[nz + to, j * half : (j + 1) * half] = part[half:]
        base = tiles * rows
        one = jnp.sum(total[base : base + 3], axis=0, keepdims=True)
        two = jnp.sum(total[base + 3 : base + 6], axis=0, keepdims=True)
        sums.append(jnp.concatenate([one, two], axis=1))
    extra = jnp.concatenate(sums, axis=0)
    extra = pltpu.roll(extra, at_ref[0], 0).astype(BF16)
    for k in range(2 * nz):
        out_ref[k, ends : ends + 8] = extra[:, :LANES]
        out_ref[k, ends + 8 :] = extra[:, LANES:]


def ring_kernel(got_ref, out_ref, short_ref, sum_ref):
    half, units = out_ref.shape
    tiles = units // LANES
    total = got_ref[0].astype(F32)
    for k in range(1, got_ref.shape[0]):
        total = total + got_ref[k].astype(F32)
    for j in range(tiles):
        part = total[j * half : (j + 1) * half]
        out_ref[:, j * LANES : (j + 1) * LANES] = part
        short_ref[:, j * LANES : (j + 1) * LANES] = part.astype(BF16)
    ends = tiles * half
    for k in range(sum_ref.shape[0]):
        sum_ref[k, :, :LANES] = total[ends : ends + 8]
        sum_ref[k, :, LANES:] = total[ends + 8 :]


def chip_kernel(mine_ref, theirs_ref, *out_refs):
    for k, out_ref in enumerate(out_refs):
        out_ref[...] = (mine_ref[k].astype(F32) + theirs_ref[k].astype(F32)).astype(BF16)


def finish_kernel(at_ref, got0, got1, got2, got3, x_ref, c_ref, gain_ref, out_ref, dn_ref):
    nz, _, cols = got0.shape
    for d in range(nz):
        own = pl.ds(pl.multiple_of(((at_ref[0] + d) % nz) * cols, cols), cols)
        total = got0[d].astype(F32)
        for got in (got1, got2, got3):
            total = total + got[d].astype(F32)
        dn_ref[:, own] = total.astype(BF16)
    v = x_ref[...].astype(F32)
    inv = lax.rsqrt(jnp.mean(v * v, axis=-1, keepdims=True) + EPS)
    xhat = v * inv
    dn = dn_ref[...].astype(F32)
    gs = gain_ref[...] * dn
    m = jnp.mean(gs * xhat, axis=-1, keepdims=True)
    out_ref[...] = (c_ref[...].astype(F32) + inv * (gs - xhat * m)).astype(BF16)


def place_kernel(at_ref, p0, p1, p2, p3, other_ref, out_ref):
    n = 4
    part = out_ref.shape[0] // (2 * n)
    for k, piece in enumerate((p0, p1, p2, p3)):
        spot = (at_ref[2] + k) % n
        own = pl.multiple_of((at_ref[1] * n + spot) * part, part)
        far = pl.multiple_of(((1 - at_ref[1]) * n + spot) * part, part)
        out_ref[pl.ds(own, part), :] = piece[:part]
        out_ref[pl.ds(far, part), :] = other_ref[k, :part]


def near(*arrays):
    return [pltpu.with_memory_space_constraint(a, pltpu.VMEM) for a in arrays]


def vmem(n):
    return [pl.BlockSpec(memory_space=pltpu.VMEM)] * n


def work(inputs, gain, gate_weight, up_weight, down_weight, cotangent):
    nz, ny, nx = lax.axis_size("fs_0"), lax.axis_size("fs_1"), lax.axis_size("x")
    rep, zl = lax.axis_index("rep"), lax.axis_index("fs_0")
    x, c = lax.axis_index("x"), lax.axis_index("c")
    tokens, width = inputs.shape
    rows, units = gate_weight.shape
    cols = width // nz
    part = tokens // 2 // nx
    gain2 = gain[None]
    at = jnp.stack([zl, c, x]).astype(jnp.int32)

    w = jnp.concatenate([gate_weight, up_weight, down_weight], axis=1)
    w0 = from_all(w, "fs_1").reshape(ny * rows, 3 * units)
    fwd, bwd = [w0], [w0]
    for _ in range(3):
        fwd.append(shifted(fwd[-1], RING, 1))
        bwd.append(shifted(bwd[-1], RING, -1))
    mid = cols // 2
    last_f = shifted(fwd[-1][:mid], RING, 1)
    last_b = shifted(bwd[-1][mid:], RING, -1)
    weights = [w0, bwd[1], bwd[2], bwd[3], fwd[3], fwd[2], fwd[1]]

    def spot(i, at):
        return ((i // nx + at[1]) % 2) * nx + (i + at[2]) % nx

    xr, own_x = pl.pallas_call(
        prepare_tokens,
        out_shape=(
            jax.ShapeDtypeStruct((nz, tokens, cols), BF16),
            jax.ShapeDtypeStruct((part, width), BF16),
        ),
        grid_spec=pltpu.PrefetchScalarGridSpec(
            num_scalar_prefetch=1,
            grid=(2 * nx,),
            in_specs=[
                pl.BlockSpec((part, width), lambda i, at: (spot(i, at), 0)),
                pl.BlockSpec((1, width), lambda i, at: (0, 0)),
            ],
            out_specs=(
                pl.BlockSpec((nz, part, cols), lambda i, at: (0, i, 0)),
                pl.BlockSpec((part, width), lambda i, at: (0, 0)),
            ),
        ),
        name="prepare_x",
    )(at, inputs, gain2)
    cr, ct, own_c = pl.pallas_call(
        prepare_cotangent,
        out_shape=(
            jax.ShapeDtypeStruct((nz, tokens, cols), BF16),
            jax.ShapeDtypeStruct((nz, cols, tokens), BF16),
            jax.ShapeDtypeStruct((part, width), BF16),
        ),
        grid_spec=pltpu.PrefetchScalarGridSpec(
            num_scalar_prefetch=1,
            grid=(nx,),
            in_specs=[
                pl.BlockSpec((part, width), lambda i, at: (spot(2 * i, at), 0)),
                pl.BlockSpec((part, width), lambda i, at: (spot(2 * i + 1, at), 0)),
            ],
            out_specs=(
                pl.BlockSpec((nz, 2 * part, cols), lambda i, at: (0, i, 0)),
                pl.BlockSpec((nz, cols, 2 * part), lambda i, at: (0, 0, i)),
                pl.BlockSpec((part, width), lambda i, at: (0, 0)),
            ),
        ),
        name="prepare_c",
    )(at, cotangent, cotangent)

    gain_ring = rolled(gain.reshape(nz, 1, cols), zl)
    acc = pl.pallas_call(
        forward_kernel,
        out_shape=jax.ShapeDtypeStruct((tokens, 3 * units), F32),
        in_specs=vmem(7),
        out_specs=pl.BlockSpec(memory_space=pltpu.VMEM),
        name="forward",
    )(xr, cr, w0, bwd[1], fwd[1], bwd[2], fwd[2])
    anywhere = pl.BlockSpec(memory_space=pl.ANY)
    mine, other, dd = pl.pallas_call(
        grad_kernel,
        out_shape=(
            jax.ShapeDtypeStruct((nx, nz, part, cols), BF16),
            jax.ShapeDtypeStruct((nx, nz, part, cols), BF16),
            jax.ShapeDtypeStruct((ny, nz, TILES * rows + 8, LANES), BF16),
        ),
        in_specs=vmem(3) + [anywhere] * 11,
        out_specs=(anywhere,) * 3,
        scratch_shapes=[
            pltpu.VMEM((tokens, 3 * units), F32),
            pltpu.VMEM((nz, tokens, cols), BF16),
            pltpu.VMEM((3, tokens, cols), BF16),
            pltpu.VMEM((nz, cols, tokens), BF16),
            pltpu.VMEM((2, cols, 3 * units), BF16),
            pltpu.VMEM((5, cols, 2 * units), BF16),
            pltpu.VMEM((2 * nx, nz, part, cols), BF16),
            pltpu.VMEM((ny, nz, TILES * rows + 8, LANES), BF16),
            pltpu.SemaphoreType.DMA((48,)),
        ],
        name="grad",
    )(gain_ring, *near(last_f, last_b), acc, xr, cr, ct, *weights)
    theirs = shifted(other, "c", 1)
    dy = exchanged(dd, "fs_1")

    chunk = jax.ShapeDtypeStruct((nz, part, cols), BF16)
    chip = pl.pallas_call(
        chip_kernel,
        out_shape=(chunk,) * 4,
        in_specs=vmem(2),
        out_specs=tuple(vmem(4)),
        compiler_params=pltpu.CompilerParams(vmem_limit_bytes=48 << 20),
        name="chip",
    )(mine, *near(theirs))
    got = [chip[0]]
    for k in (1, 2, 3):
        got.append(shifted(chip[k], "x", k))
    ig = pl.pallas_call(
        finish_kernel,
        out_shape=jax.ShapeDtypeStruct((part, width), BF16),
        grid_spec=pltpu.PrefetchScalarGridSpec(
            num_scalar_prefetch=1,
            grid=(1,),
            in_specs=vmem(7),
            out_specs=pl.BlockSpec((part, width), lambda i, at: (0, 0)),
            scratch_shapes=[pltpu.VMEM((part, width), BF16)],
        ),
        name="finish",
    )(at, got[0], *near(*got[1:]), own_x, own_c, gain2)
    pieces = [ig]
    for k in (1, 2, 3):
        pieces.append(shifted(ig, "x", -k))
    ig_other = shifted(jnp.stack(pieces), "c", 1)
    out = pl.pallas_call(
        place_kernel,
        out_shape=jax.ShapeDtypeStruct((tokens, width), BF16),
        in_specs=[pl.BlockSpec(memory_space=pltpu.SMEM)] + vmem(5),
        out_specs=pl.BlockSpec(memory_space=pltpu.VMEM),
        name="place",
    )(at, pieces[0], *near(*pieces[1:], ig_other))

    dz = pl.pallas_call(
        rows_kernel,
        out_shape=jax.ShapeDtypeStruct((2 * nz, TILES * rows // 2 + 16, LANES), BF16),
        in_specs=[pl.BlockSpec(memory_space=pltpu.SMEM)] + vmem(1),
        out_specs=pl.BlockSpec(memory_space=pltpu.VMEM),
        name="ysum",
    )(at, *near(dy))
    dz = exchanged(dz, RING)
    own, short, gain_own = pl.pallas_call(
        ring_kernel,
        out_shape=(
            jax.ShapeDtypeStruct((rows // 2, units), F32),
            jax.ShapeDtypeStruct((rows // 2, units), BF16),
            jax.ShapeDtypeStruct((lax.axis_size(TP), nz, cols), F32),
        ),
        in_specs=vmem(1),
        out_specs=tuple(vmem(3)),
        name="zsum",
    )(*near(dz))
    gain_all = exchanged(gain_own, TP)
    gain_gradient = jnp.sum(gain_all, axis=0).reshape(width)
    far = shifted(short, "rep", 1).astype(F32)
    pair = rolled(jnp.stack([own, far]), rep)
    d_down = pair.reshape(rows, units)
    return (out, gain_gradient, d_down)


def solution(mesh):
    torus = Mesh(
        mesh.devices.reshape(mesh.shape["rep"], 8, 4, 4, 2),
        ("rep", "fs_0", "fs_1", "x", "c"),
    )
    return jax.shard_map(
        work,
        mesh=torus,
        in_specs=(P(REP_FS, None), P(), P(FS, TP), P(FS, TP), P(FS, TP), P(REP_FS, None)),
        out_specs=(P(REP_FS, None), P(), P(FS, TP)),
        check_vma=False,
    )
```
